32 devices in a mesh: sp: 8 (over z, x), tp: 4 (over y, core).
Axes of the slice: x: 2, y: 2, z: 4, core: 2. Of those that a mesh axis runs over, the one named last changes fastest.
Arguments:
- cotangent: bfloat16 [2048, 2048], P('sp', 'tp'), may hold values from -6 to 6
- moe_input: bfloat16 [2048, 2048], P('sp', 'tp'), may hold values from -6 to 6
- routes: int32 [2048, 2], P('sp'), may hold values from 0 to 7, all different within a row; in each aligned block of 256 rows (0 to 255, 256 to 511, ...) at most 96 rows name the same one
- gates: float32 [2048, 2], P('sp'), may hold values from 0.1 to 1
- w_gate: bfloat16 [8, 2048, 2048], P('sp', None, 'tp'), may hold values from -0.125 to 0.125
- w_up: bfloat16 [8, 2048, 2048], P('sp', None, 'tp'), may hold values from -0.125 to 0.125
- w_down: bfloat16 [8, 2048, 2048], P('sp', 'tp'), may hold values from -0.125 to 0.125
- out_proj: bfloat16 [1024, 2048], P('tp'), may hold values from -0.1875 to 0.1875
- conv_in: bfloat16 [1024, 2048], P('tp', 'sp'), may hold values from -6 to 6
- branch: bfloat16 [1024, 2048], P('tp', 'sp'), may hold values from -6 to 6
- state_before: float32 [1024, 2048], P('tp', 'sp'), may hold values from -6 to 6
- state_after: float32 [1024, 2048], P('tp', 'sp'), may hold values from -6 to 6
- jump: float32 [1024, 2048], P('tp', 'sp'), may hold values from -2 to 0, as said below
- recur_weight: bfloat16 [2, 16, 64, 64], P(None, 'tp'), may hold values from -0.75 to 0.75
- input_weight: bfloat16 [2, 16, 64, 64], P(None, 'tp'), may hold values from -0.75 to 0.75
- lam: float32 [2, 1024], P(None, 'tp')
Outputs:
- gate_grad: bfloat16 [8, 2048, 2048], P('sp', None, 'tp')
- up_grad: bfloat16 [8, 2048, 2048], P('sp', None, 'tp')
- down_grad: bfloat16 [8, 2048, 2048], P('sp', 'tp')
- residual_grad: bfloat16 [2048, 2048], P('sp', 'tp')
- out_proj_grad: float32 [1024, 2048], P('tp', 'sp')
- conv_grad: float32 [1024, 2048], P('tp', 'sp')
- branch_grad: float32 [1024, 2048], P('tp', 'sp')
The draws below stay inside these ranges and needn't reach their ends.
Inputs may be any that keep to these rules, and one draw needn't show every extreme that they name: `routes`: each token names 2 different experts. Among the tokens of one index of sp (aligned blocks of 256 rows) no expert is named more than 96 times, a bound that some block reaches. `jump`: every entry is at most -1 / 20480.
All inputs are finite; a program needn't handle non-finite values.
Results may differ from the reference program's by a relative error of at most 0.02.
Values may be sent and summed in bfloat16 or wider, within the bound.
A program may use at most 128 MiB of HBM per device.

```python
import math
import jax
import jax.numpy as jnp
import numpy as np
from jax import lax

D = 2048
RECURRENT_WIDTH = 1024
BW = 64
BLOCKS = 16
FFE = 2048
TOP = 2
TOK_DEV = 256
EXPERTS = 8
SEQUENCE_TOKENS = 2048
CAP = 96
N_SP = 8
N_TP = 4


def draw_lam(key, part):
    k_fast, k_span, k_slow = jax.random.split(jax.random.fold_in(key, 11), 3)
    fast_share = 0.5
    is_fast = jax.random.uniform(k_fast, (2, RECURRENT_WIDTH), jnp.float32) < fast_share
    fast_len = jax.random.uniform(k_span, (2, RECURRENT_WIDTH), jnp.float32, 30.0, 100.0)
    slow_len = SEQUENCE_TOKENS * jax.random.uniform(k_slow, (2, RECURRENT_WIDTH), jnp.float32, 1.0, 2.0)
    length = jnp.where(is_fast, fast_len, slow_len)
    step_rate = 2.0 / (8.0 * length)
    return -jnp.log(jnp.expm1(step_rate))


def draw_jump(key, part):
    folded = jax.random.fold_in(key, 23)
    k_rate, k_cell, random_location, random_extent = jax.random.split(folded, 4)
    blocks = SEQUENCE_TOKENS // TOK_DEV
    block_rate = jnp.exp(jax.random.uniform(k_rate, (blocks,), jnp.float32, math.log(0.2), math.log(0.8)))
    cell_multiplier = jnp.exp(jax.random.uniform(k_cell, (RECURRENT_WIDTH, SEQUENCE_TOKENS), jnp.float32, math.log(0.5), math.log(2.0)))
    token_position = jnp.arange(SEQUENCE_TOKENS, dtype=jnp.int32)
    position_values = jnp.repeat(block_rate, TOK_DEV) / SEQUENCE_TOKENS
    spike_offset = jax.random.randint(random_location, (2,), 0, SEQUENCE_TOKENS)
    spike_mask = ((token_position == spike_offset[0]) | (token_position == spike_offset[1])).astype(jnp.float32)[None, :]
    spike_extent = jnp.log(jax.random.uniform(random_extent, (RECURRENT_WIDTH, 1), jnp.float32, 0.55, 0.8))
    return -position_values[None, :] * cell_multiplier + spike_mask * spike_extent


def spiked(values, own_key, source, target, parts, factor):
    def block_of(position):
        return (jnp.arange(values.shape[position]) // (values.shape[position] // parts)).reshape((-1,) + (1,) * (values.ndim - 1 - position))

    first = jax.random.permutation(own_key, parts)[block_of(target)]
    second = (block_of(target) + parts // 2) % parts
    return jnp.where((block_of(source) == first) | (block_of(source) == second), factor * values, values)


def levels(rng, extent, cuts, least, high):
    loudness = 1.0
    for dim, parts in cuts:
        steps = jax.random.uniform(jax.random.fold_in(jax.random.fold_in(rng, 6), dim), (parts,), jnp.float32, least / len(cuts), high / len(cuts))
        loudness = loudness * jnp.repeat(jnp.exp(steps), extent[dim] // parts).reshape((-1,) + (1,) * (len(extent) - 1 - dim))
    return loudness


def assign_block(rng, own, number, rows, number_of, top, most, skew):
    sequence = jax.random.permutation(rng, number_of)
    heavy_load, ordinary = load_shares(number_of, rows * top, most, skew, True), load_shares(number_of, rows * top, most, skew, False)
    places = jnp.arange(number_of)

    def named(sizes, turn):
        used = int((sizes > 0).sum())
        fixed = max(1, used // 4)
        shifted = fixed + (places - fixed + turn * (used - fixed)) % max(1, number_of - fixed)
        return jnp.zeros((number_of,), jnp.int32).at[sequence[jnp.where(places < fixed, places, shifted)]].set(jnp.asarray(sizes, jnp.int32))

    sizes = jnp.where(number % 4 == 0, named(heavy_load, number // 4), named(ordinary, number - number // 4 - 1))
    mixed = jax.random.permutation(jax.random.fold_in(own, 3), number_of)
    donor, receiver = mixed[0:number_of // 2 * 2:2], mixed[1:number_of // 2 * 2:2]
    margin = jnp.minimum(sizes[donor] - 1, most - sizes[receiver]) // 2
    margin = jnp.where((donor == sequence[0]) | (receiver == sequence[0]) | (sizes[receiver] == 0), 0, jnp.maximum(margin, 0))
    shifted = jax.random.randint(jax.random.fold_in(own, 4), (number_of // 2,), 0, 1 << 20) % (margin + 1)
    sizes = sizes.at[donor].add(-shifted).at[receiver].add(shifted)
    items = jnp.searchsorted(jnp.cumsum(sizes), jnp.arange(rows * top), side="right").astype(jnp.int32)
    listing = items.reshape(top, rows).T
    listing = listing[jax.random.permutation(jax.random.fold_in(own, 1), rows)]
    turn = jax.random.randint(jax.random.fold_in(own, 2), (rows, 1), 0, top)
    return jnp.take_along_axis(listing, (jnp.arange(top)[None, :] + turn) % top, axis=1)


def load_shares(number_of, total, most, lean, full):
    portions = [(1 << 20) // math.isqrt(grade ** lean) + 1 for grade in range(1, number_of + 1)]
    largest = most if full else min(most, max(-(-total // number_of), total * portions[0] // sum(portions)))
    least = 1 if total - largest >= number_of - 1 else 0
    given, surplus = [largest] + [least] * (number_of - 1), total - largest - least * (number_of - 1)
    while surplus > 0:
        free = [i for i in range(1, number_of) if given[i] < largest] or [i for i in range(1, number_of) if given[i] < most]
        whole, remaining = sum([portions[i] for i in free]), surplus
        for i in free:
            extra = min(most - given[i], max(1, remaining * portions[i] // whole), surplus)
            given[i] = given[i] + extra
            surplus = surplus - extra
    return np.array(given)


def bell_draw(rng, shape, spread, limit, cuts=(), kind=jnp.bfloat16):
    array = spread * jax.random.normal(rng, shape, jnp.float32)
    if cuts:
        array = array * levels(rng, shape, cuts, -0.22, 0.18)
    return jnp.clip(array, -limit, limit).astype(kind)


def gaussian_with(key, dims, scale, most, cuts, heavy, kind=jnp.bfloat16):
    array = scale * jax.random.normal(key, dims, jnp.float32)
    if cuts:
        array = array * levels(key, dims, cuts, -0.22, 0.18)
    return jnp.clip(spiked(array, jax.random.fold_in(key, 3), *heavy), -most, most).astype(kind)


def setup_inputs(seed: int = 0) -> dict:
    key_list = jax.random.split(jax.random.key(seed), 17)
    cotangent = gaussian_with(key_list[0], (SEQUENCE_TOKENS, D), 1.0, 6.0, ((0, 8), (1, 4)), (0, 1, 8, 2.0))
    moe_input = bell_draw(key_list[1], (SEQUENCE_TOKENS, D), 1.0, 6.0, ((0, 8), (1, 4)))
    routes_keys = jax.random.split(jax.random.fold_in(key_list[2], 1), SEQUENCE_TOKENS // TOK_DEV)
    routes_turns = jax.random.permutation(jax.random.fold_in(key_list[2], 3), SEQUENCE_TOKENS // TOK_DEV)
    routes = jax.vmap(lambda own, number: assign_block(jax.random.fold_in(key_list[2], 2), own, number, TOK_DEV, EXPERTS, TOP, CAP, 1))(routes_keys, routes_turns).reshape((SEQUENCE_TOKENS, TOP))
    gates = jnp.clip(0.1 + 0.9 * jax.random.uniform(key_list[3], (SEQUENCE_TOKENS, TOP), jnp.float32) ** levels(key_list[3], (SEQUENCE_TOKENS, TOP), ((0, 8),), -0.2, 0.2), 0.1, 1.0)
    w_gate = bell_draw(key_list[4], (EXPERTS, D, FFE), D ** -0.5, 0.125, ((0, 8), (2, 4)))
    w_up = bell_draw(key_list[5], (EXPERTS, D, FFE), D ** -0.5, 0.125, ((0, 8), (2, 4)))
    w_down = bell_draw(key_list[6], (EXPERTS, FFE, D), FFE ** -0.5, 0.125, ((0, 8), (1, 4)))
    out_proj = bell_draw(key_list[7], (RECURRENT_WIDTH, D), RECURRENT_WIDTH ** -0.5, 0.1875, ((0, 4),))
    conv_in = bell_draw(key_list[8], (RECURRENT_WIDTH, SEQUENCE_TOKENS), 1.0, 6.0, ((0, 4), (1, 8)))
    branch = bell_draw(key_list[9], (RECURRENT_WIDTH, SEQUENCE_TOKENS), 1.0, 6.0, ((0, 4), (1, 8)))
    state_before = bell_draw(key_list[10], (RECURRENT_WIDTH, SEQUENCE_TOKENS), 1.0, 6.0, ((0, 4), (1, 8)), jnp.float32)
    state_after = bell_draw(key_list[11], (RECURRENT_WIDTH, SEQUENCE_TOKENS), 1.0, 6.0, ((0, 4), (1, 8)), jnp.float32)
    jump = draw_jump(jax.random.fold_in(key_list[16], 71), 0)
    recur_weight = bell_draw(key_list[13], (2, BLOCKS, BW, BW), BW ** -0.5, 0.75, ((1, 4),))
    input_weight = bell_draw(key_list[14], (2, BLOCKS, BW, BW), BW ** -0.5, 0.75, ((1, 4),))
    lam = draw_lam(jax.random.fold_in(key_list[16], 71), 0)
    return {"cotangent": cotangent, "moe_input": moe_input, "routes": routes, "gates": gates, "w_gate": w_gate, "w_up": w_up, "w_down": w_down, "out_proj": out_proj, "conv_in": conv_in, "branch": branch, "state_before": state_before, "state_after": state_after, "jump": jump, "recur_weight": recur_weight, "input_weight": input_weight, "lam": lam}


decay_scale = 8.0

def silu_parts(pre_act):
    sigmoid_val = jax.nn.sigmoid(pre_act)
    return (pre_act * sigmoid_val, sigmoid_val * (1.0 + pre_act * (1.0 - sigmoid_val)))

def block_map(values, weight):
    return jnp.einsum('nit,nij->njt', values.astype(jnp.float32), weight.astype(jnp.float32), precision=lax.Precision.HIGHEST)

def block_back(gradient, weight):
    return jnp.einsum('njt,nij->nit', gradient, weight.astype(jnp.float32), precision=lax.Precision.HIGHEST)

def gate_values(conv_in, weight_r, weight_i, lam_row, jump):
    channels, length = conv_in.shape
    shaped = conv_in.reshape(weight_r.shape[0], weight_r.shape[1], length)
    recur_gate = jax.nn.sigmoid(block_map(shaped, weight_r).reshape(channels, length))
    inward = jax.nn.sigmoid(block_map(shaped, weight_i).reshape(channels, length))
    speed_row = decay_scale * jax.nn.softplus(-lam_row)[:, None]
    log_decay = -speed_row * recur_gate + jump
    retain = jnp.exp(log_decay)
    root_term = jnp.sqrt(-jnp.expm1(2.0 * log_decay))
    conv_wide = conv_in.astype(jnp.float32)
    return (recur_gate, inward, speed_row, retain, root_term, conv_wide)

def gate_backward(pieces, decay_grad, drive_grad, weight_r, weight_i):
    recur_gate, inward, speed_row, retain, root_term, conv_wide = pieces
    channels, length = conv_wide.shape
    shape_three = (weight_r.shape[0], weight_r.shape[1], length)
    log_grad = decay_grad * retain - drive_grad * inward * conv_wide * retain * retain / root_term
    recur_grad = log_grad * -speed_row * recur_gate * (1.0 - recur_gate)
    inward_grad = drive_grad * root_term * conv_wide * inward * (1.0 - inward)
    direct = drive_grad * root_term * inward
    back_r = block_back(recur_grad.reshape(shape_three), weight_r)
    back_i = block_back(inward_grad.reshape(shape_three), weight_i)
    return direct + (back_r + back_i).reshape(channels, length)

def combine_pair(earlier, latter):
    return (earlier[0] * latter[0], latter[0] * earlier[1] + latter[1])

def expert_terms(routed_rows, routed_grads, gate_weight, up_weight, down_weight):
    pre_gate = jnp.dot(routed_rows, gate_weight, preferred_element_type=jnp.float32)
    pre_up = jnp.dot(routed_rows, up_weight, preferred_element_type=jnp.float32)
    silu_val, silu_slope = silu_parts(pre_gate)
    activation = (silu_val * pre_up).astype(jnp.bfloat16)
    act_grad = jnp.dot(routed_grads, down_weight.T, preferred_element_type=jnp.float32)
    up_hidden = (act_grad * silu_val).astype(jnp.bfloat16)
    gate_hidden = (act_grad * pre_up * silu_slope).astype(jnp.bfloat16)
    down_acc = jnp.dot(activation.T, routed_grads, preferred_element_type=jnp.float32)
    gate_acc = jnp.dot(routed_rows.T, gate_hidden, preferred_element_type=jnp.float32)
    up_acc = jnp.dot(routed_rows.T, up_hidden, preferred_element_type=jnp.float32)
    return (gate_hidden, up_hidden, gate_acc, up_acc, down_acc)

def reference(cotangent, moe_input, routes, gates, w_gate, w_up, w_down, out_proj, conv_in, branch, state_before, state_after, jump, recur_weight, input_weight, lam):
    per_token = routes.shape[1]
    routed = routes.reshape(-1)
    pair_total = routed.shape[0]
    scaled = (cotangent.astype(jnp.float32)[:, None, :] * gates[:, :, None]).astype(jnp.bfloat16)
    scaled = scaled.reshape(pair_total, D)
    copies = jnp.broadcast_to(moe_input[:, None, :], (SEQUENCE_TOKENS, per_token, D)).reshape(pair_total, D)
    zero_row = jnp.zeros((1, D), jnp.bfloat16)
    padded_rows = jnp.concatenate([copies, zero_row], axis=0)
    padded_grads = jnp.concatenate([scaled, zero_row], axis=0)
    buffer_rows = N_SP * CAP
    per_dev = FFE // N_TP

    def one_expert(returned, inputs):
        gate_weight, up_weight, down_weight, expert = inputs
        chosen = jnp.nonzero(routed == expert, size=buffer_rows, fill_value=pair_total)[0].astype(jnp.int32)
        routed_rows = padded_rows[chosen]
        routed_grads = padded_grads[chosen]
        gate_hidden, up_hidden, gate_acc, up_acc, down_acc = expert_terms(routed_rows, routed_grads, gate_weight, up_weight, down_weight)
        split_gate = jnp.einsum('rkf,dkf->krd', gate_hidden.astype(jnp.float32).reshape(buffer_rows, N_TP, per_dev), gate_weight.astype(jnp.float32).reshape(D, N_TP, per_dev), precision=lax.Precision.HIGHEST)
        split_up = jnp.einsum('rkf,dkf->krd', up_hidden.astype(jnp.float32).reshape(buffer_rows, N_TP, per_dev), up_weight.astype(jnp.float32).reshape(D, N_TP, per_dev), precision=lax.Precision.HIGHEST)
        partial_value = (split_gate + split_up).astype(jnp.bfloat16)
        partial_value = lax.optimization_barrier(partial_value)
        row_grad = lax.optimization_barrier(jnp.sum(partial_value.astype(jnp.float32), axis=0)).astype(jnp.bfloat16)
        returned = returned.at[chosen].set(row_grad)
        return (returned, (gate_acc.astype(jnp.bfloat16), up_acc.astype(jnp.bfloat16), down_acc.astype(jnp.bfloat16)))
    start = jnp.zeros((pair_total + 1, D), jnp.bfloat16)
    returned, grads_all = lax.scan(one_expert, start, (w_gate, w_up, w_down, jnp.arange(EXPERTS, dtype=jnp.int32)))
    gate_grad, up_grad, down_grad = grads_all
    backward_rows = returned[:pair_total].reshape(SEQUENCE_TOKENS, per_token, D)
    residual_grad = (cotangent.astype(jnp.float32) + lax.optimization_barrier(jnp.sum(backward_rows.astype(jnp.float32), axis=1))).astype(jnp.bfloat16)
    mix_grad = jnp.dot(out_proj, residual_grad.T, preferred_element_type=jnp.float32)
    pieces_fwd = gate_values(conv_in, recur_weight[0], input_weight[0], lam[0], jump)
    pieces_bwd = gate_values(conv_in, recur_weight[1], input_weight[1], lam[1], jump)
    drive_fwd = pieces_fwd[4] * pieces_fwd[1] * pieces_fwd[5]
    drive_bwd = pieces_bwd[4] * pieces_bwd[1] * pieces_bwd[5]
    lru_out = pieces_fwd[3] * state_before + drive_fwd + pieces_bwd[3] * state_after + drive_bwd
    gelu_val, gelu_back = jax.vjp(jax.nn.gelu, branch.astype(jnp.float32))
    mix = (lru_out * gelu_val).astype(jnp.bfloat16)
    out_proj_grad = jnp.dot(mix, residual_grad, preferred_element_type=jnp.float32)
    lru_grad = mix_grad * gelu_val
    branch_grad = gelu_back(mix_grad * lru_out)[0]
    decay_fwd = pieces_fwd[3]
    decay_bwd = pieces_bwd[3]
    carried_fwd = lax.associative_scan(combine_pair, (decay_fwd, decay_fwd * lru_grad), reverse=True, axis=1)[1]
    carried_bwd = lax.associative_scan(combine_pair, (decay_bwd, decay_bwd * lru_grad), axis=1)[1]
    zeros_col = jnp.zeros((RECURRENT_WIDTH, 1), jnp.float32)
    delta_fwd = lru_grad + jnp.concatenate([carried_fwd[:, 1:], zeros_col], axis=1)
    delta_bwd = lru_grad + jnp.concatenate([zeros_col, carried_bwd[:, :-1]], axis=1)
    conv_grad = gate_backward(pieces_fwd, delta_fwd * state_before, delta_fwd, recur_weight[0], input_weight[0])
    conv_grad = conv_grad + gate_backward(pieces_bwd, delta_bwd * state_after, delta_bwd, recur_weight[1], input_weight[1])
    return (gate_grad, up_grad, down_grad, residual_grad, out_proj_grad, conv_grad, branch_grad)
```

```python
import jax
import jax.numpy as jnp
from jax import lax
from jax.experimental import pallas as pl
from jax.experimental.pallas import tpu as pltpu
from jax.sharding import PartitionSpec as P

decay_scale = 8.0


MESH = pl.DeviceIdType.MESH
VMEM_SPEC = pl.BlockSpec(memory_space=pltpu.VMEM)


def at(sp=None, tp=None):
    sp = lax.axis_index("sp") if sp is None else sp
    tp = lax.axis_index("tp") if tp is None else tp
    return (sp, tp)


def meet(devices):
    barrier = pltpu.get_barrier_semaphore()
    for device in devices:
        pl.semaphore_signal(barrier, inc=1, device_id=device, device_id_type=MESH)
    pl.semaphore_wait(barrier, len(devices))


def remote(source, target, send, recv, device):
    return pltpu.make_async_remote_copy(
        src_ref=source, dst_ref=target, send_sem=send, recv_sem=recv,
        device_id=device, device_id_type=MESH,
    )


def softplus(value):
    small = jnp.exp(-jnp.abs(value))
    series = small * (1.0 - small * (0.5 - small * (1.0 / 3.0 - small * 0.25)))
    return jnp.maximum(value, 0.0) + jnp.where(small < 0.01, series, jnp.log(1.0 + small))


def one_minus_exp(value, exponential):
    series = -value * (
        1.0 + value * (0.5 + value * (1.0 / 6.0 + value * (1.0 / 24.0 + value * (
            1.0 / 120.0 + value * (1.0 / 720.0)
        ))))
    )
    return jnp.where(value > -0.25, series, 1.0 - exponential)


def layer_backward(
    cotangent, moe_input, routes, gates, w_gate, w_up, w_down, out_proj, conv_in, branch,
    state_before, state_after, jump, recur_weight, input_weight, lam,
):
    n, tp = lax.axis_size("sp"), lax.axis_size("tp")
    chips = tp // 2
    tokens, width = cotangent.shape
    full_width, hidden = w_gate.shape
    cap = -(-(3 * tokens // n) // 16) * 16
    span = min(n, 2 if n <= 8 else 4)
    groups = n // span
    fine = span if n <= 8 else 1
    per_unit = span // fine
    units = groups * fine
    chunk = span * cap
    total_rows = n * cap
    hidden_block = min(hidden, 256)
    column_block = min(full_width, 512)
    grad_block = min(full_width, 256)
    f32, bf16 = jnp.float32, jnp.bfloat16
    channels, length = conv_in.shape
    blocks, block_width = recur_weight.shape[1:3]
    channels_pad = max(channels, 128)
    strip = full_width // n
    upright = strip % 128 == 0
    levels = [1 << i for i in range((length - 1).bit_length())]

    def kernel(
        cot_ref, in_ref, routes_ref, gates_ref, conv_ref, branch_ref, before_ref, after_ref,
        jump_ref, wr_ref, wi_ref, lam_ref, outp_ref, wg_hbm, wu_hbm, wd_hbm,
        res_ref, proj_ref, conv_out, branch_out, gate_hbm, up_hbm, down_hbm,
        wg, wu, wd, key_t, gate_t, pick, send, full, hid, act, part, near, total, far, ret, rets,
        gate_out, up_out, down_out, fullres_ref,
        slopes, steps, decay, tails, speed, mix, gelu_val, gelu_slope, mix_grad, local,
        ends, ends_row, ends_all, carry, proj_part, proj_near, proj_sum, proj_far,
        es, er, xs, xr, zs, zr,
        ws, ss, sr, ys, yr, ps, pr, fs, fr, ns, nr, ts, tr, bs, br, gs, gr, hs, hr, os,
    ):
        me, place = lax.axis_index("sp"), lax.axis_index("tp")
        chip, core = place // 2, place % 2
        partner = chip * 2 + (1 - core)
        group, inner = me // span, me % span

        def columns(member):
            return pl.ds(pl.multiple_of(member * width, width), width)

        mine = columns(place)

        def turned(t, sign):
            return lax.rem(chip + sign * t + chips, chips)

        def across(t, sign):
            return turned(t, sign) * 2 + core

        def order(j):
            return jnp.where(j < 2, j, groups + 1 - j)

        def group_of(j, sign):
            return lax.rem(group + sign * order(j) + groups, groups)

        def peer(j, i, sign):
            return group_of(j, sign) * span + lax.rem(inner + sign * i + span, span)

        weights = ((wg_hbm, wg), (wu_hbm, wu), (wd_hbm, wd))
        loads = [pltpu.make_async_copy(a, b, ws.at[i]) for i, (a, b) in enumerate(weights)]
        for load in loads:
            load.start()

        meet(
            [at(sp=lax.rem(me + k, n)) for k in range(1, n)]
            + [at(tp=partner)]
            + [at(tp=across(t, 1)) for t in range(1, chips)]
        )

        lanes = lax.broadcasted_iota(jnp.int32, (tokens, 128), 1)
        first = lanes == routes_ref[:, 0:1]
        second = lanes == routes_ref[:, 1:2]
        member = jnp.where(first | second, 1.0, 0.0).astype(f32)
        weight = jnp.where(first, gates_ref[:, 0:1], 0.0) + jnp.where(second, gates_ref[:, 1:2], 0.0)
        below = lax.broadcasted_iota(jnp.int32, (tokens, tokens), 1) < lax.broadcasted_iota(
            jnp.int32, (tokens, tokens), 0
        )
        below = jnp.where(below, 1.0, 0.0).astype(bf16)
        position = jnp.dot(below, member.astype(bf16), preferred_element_type=f32)
        key_t[...] = jnp.where(member > 0.5, position, -1.0).T
        gate_t[...] = weight.T
        row_id = lax.broadcasted_iota(jnp.int32, (cap, tokens), 0).astype(f32)

        def packed(to):
            chosen = row_id == key_t[pl.ds(to, 1), :]
            one_hot = jnp.where(chosen, 1.0, 0.0).astype(bf16)
            scale = jnp.sum(jnp.where(chosen, gate_t[pl.ds(to, 1), :], 0.0), axis=1, keepdims=True)
            pick[pl.ds(pl.multiple_of(to * cap, 16), cap), :] = one_hot
            rows = jnp.dot(one_hot, in_ref[...], preferred_element_type=f32).astype(bf16)
            grads = jnp.dot(one_hot, cot_ref[...], preferred_element_type=f32) * scale
            return rows, grads.astype(bf16)

        rows, grads = packed(me)
        full[me, 0, :, mine] = rows
        full[me, 1, :, mine] = grads

        def unit_slice(j, i):
            base = group_of(j, -1) * span
            if fine > 1:
                return pl.ds(base + lax.rem(inner - i + span, span), 1)
            return pl.ds(base, span)

        def dispatch_copy(j, i, sign):
            other = peer(j, i, sign)
            k = j * span + i
            return remote(
                send.at[other], full.at[me if sign > 0 else other, :, :, mine],
                ss.at[k], sr.at[k], at(sp=other),
            )

        def hand_over(j, i):
            block = full.at[unit_slice(j, i), :, :, mine]
            u = j * fine + i
            out = [
                remote(block, block, ys.at[u, t], yr.at[u, t], at(tp=across(t, 1)))
                for t in range(1, chips)
            ]
            out.append(remote(block, block, ps.at[u], pr.at[u], at(tp=partner)))
            return out

        def pass_on(j, i, t):
            block = full.at[unit_slice(j, i), :, :, columns(across(t, -1))]
            u = j * fine + i
            return remote(block, block, fs.at[u, t], fr.at[u, t], at(tp=partner))

        def start_forward(j, begin=0):
            for i in range(begin, fine):
                for s in range(per_unit):
                    number = i * per_unit + s

                    @pl.when(j * span + number > 0)
                    def _():
                        dispatch_copy(j, number, -1).wait_recv()

                for copy in hand_over(j, i):
                    copy.start()

        def start_pass(j):
            for i in range(fine):
                u = j * fine + i
                for t in range(1, chips):
                    block = full.at[unit_slice(j, i), :, :, columns(across(t, -1))]
                    remote(
                        block, block, ys.at[u, t], yr.at[u, t], at(tp=across(t, -1))
                    ).wait_recv()
                    pass_on(j, i, t).start()

        def end_pass(j):
            for i in range(fine):
                u = j * fine + i
                block = full.at[unit_slice(j, i), :, :, columns(partner)]
                remote(block, block, ps.at[u], pr.at[u], at(tp=partner)).wait_recv()
                for t in range(1, chips):
                    block = full.at[
                        unit_slice(j, i), :, :, columns(turned(t, -1) * 2 + (1 - core))
                    ]
                    remote(block, block, fs.at[u, t], fr.at[u, t], at(tp=partner)).wait_recv()

        def chunk_rows(j):
            return pl.ds(pl.multiple_of(group_of(j, -1) * chunk, 16), chunk)

        def near_copy(j, t):
            return remote(
                part.at[chunk_rows(j), columns(turned(t, 1) * 2 + (1 - core))],
                near.at[j, t], ns.at[j, t], nr.at[j, t], at(tp=partner),
            )

        def far_copy(j, t):
            return remote(
                total.at[j, t], far.at[j, t], ts.at[j, t], tr.at[j, t], at(tp=across(t, 1))
            )

        def compute(j):
            base = group_of(j, -1) * span
            where = chunk_rows(j)

            @pl.loop(0, hidden // hidden_block)
            def _(b):
                cut = pl.ds(pl.multiple_of(b * hidden_block, hidden_block), hidden_block)
                rows = full[pl.ds(base, span), 0].reshape(chunk, full_width)
                pre_gate = jnp.dot(rows, wg[:, cut], preferred_element_type=f32)
                pre_up = jnp.dot(rows, wu[:, cut], preferred_element_type=f32)
                grads = full[pl.ds(base, span), 1].reshape(chunk, full_width)
                act_grad = lax.dot_general(
                    grads, wd[cut, :], (((1,), (1,)), ((), ())), preferred_element_type=f32
                )
                sigmoid = jax.nn.sigmoid(pre_gate)
                silu = pre_gate * sigmoid
                slope = sigmoid * (1.0 + pre_gate * (1.0 - sigmoid))
                act[where, cut] = (silu * pre_up).astype(bf16)
                hid[0, where, cut] = (act_grad * pre_up * slope).astype(bf16)
                hid[1, where, cut] = (act_grad * silu).astype(bf16)

            @pl.loop(0, full_width // column_block)
            def _(b):
                cut = pl.ds(pl.multiple_of(b * column_block, column_block), column_block)
                value = lax.dot_general(
                    hid[0, where, :], wg[cut, :], (((1,), (1,)), ((), ())), preferred_element_type=f32
                ) + lax.dot_general(
                    hid[1, where, :], wu[cut, :], (((1,), (1,)), ((), ())), preferred_element_type=f32
                )
                part[where, cut] = value.astype(bf16)

            for t in range(chips):
                near_copy(j, t).start()

        def reduce_near(j):
            where = chunk_rows(j)
            for t in list(range(1, chips)) + [0]:
                near_copy(j, t).wait_recv()
                if t > 0:
                    value = part[where, columns(turned(t, 1) * 2 + core)].astype(f32) + near[
                        j, t
                    ].astype(f32)
                    total[j, t] = value.astype(bf16)
                    far_copy(j, t).start()

        def return_copy(j, i):
            other = peer(j, i, -1)
            k = j * span + i
            return remote(ret.at[other], rets.at[me], bs.at[k], br.at[k], at(sp=other))

        def reduce_far(j):
            where = chunk_rows(j)
            value = part[where, mine].astype(f32) + near[j, 0].astype(f32)
            for t in range(1, chips):
                far_copy(j, t).wait_recv()
                value = value + far[j, t].astype(f32)
            ret[pl.ds(group_of(j, -1) * span, span)] = value.astype(bf16).reshape(span, cap, width)
            for i in range(span):

                @pl.when(j * span + i > 0)
                def _():
                    return_copy(j, i).start()

        if fine > 1:
            for copy in hand_over(0, 0):
                copy.start()

        @pl.loop(1, n)
        def _(k):
            j, i = k // span, k % span
            to = peer(j, i, 1)
            rows, grads = packed(to)
            send[to, 0] = rows
            send[to, 1] = grads
            dispatch_copy(j, i, 1).start()

        start_forward(0, 1 if fine > 1 else 0)

        diagonal = lax.broadcasted_iota(jnp.int32, (channels, channels), 0) == (
            lax.broadcasted_iota(jnp.int32, (channels, channels), 1)
        )
        for d in range(2):
            column = jnp.sum(
                jnp.where(diagonal, lam_ref[d : d + 1, :], 0.0), axis=1, keepdims=True
            )
            speed[d] = decay_scale * softplus(-jnp.broadcast_to(column, (channels, 128)))
        token = lax.broadcasted_iota(jnp.int32, (block_width, length), 1)

        def shifted(value, by, d):
            return pltpu.roll(value, length - by if d == 0 else by, 1)

        def inside(by, d):
            return token < length - by if d == 0 else token >= by

        @pl.loop(0, blocks)
        def _(b):
            rows = pl.ds(pl.multiple_of(b * block_width, block_width), block_width)
            conv = conv_ref[rows, :]
            wide = conv.astype(f32)
            lru_out = jnp.zeros((block_width, length), f32)
            for d, state_ref in enumerate((before_ref, after_ref)):
                recur = jax.nn.sigmoid(
                    lax.dot_general(
                        wr_ref[d, b], conv, (((0,), (0,)), ((), ())), preferred_element_type=f32
                    )
                )
                inward = jax.nn.sigmoid(
                    lax.dot_general(
                        wi_ref[d, b], conv, (((0,), (0,)), ((), ())), preferred_element_type=f32
                    )
                )
                rate = speed[d, rows, 0:1]
                log_decay = jump_ref[rows, :] - rate * recur
                retain = jnp.exp(log_decay)
                root = jnp.sqrt(one_minus_exp(2.0 * log_decay, retain * retain))
                state = state_ref[rows, :]
                lru_out = lru_out + retain * state + root * inward * wide
                log_slope = state * retain - inward * wide * retain * retain / root
                slopes[d, 0, rows, :] = -rate * log_slope * recur * (1.0 - recur)
                slopes[d, 1, rows, :] = root * wide * inward * (1.0 - inward)
                slopes[d, 2, rows, :] = root * inward
                decay[d, rows, :] = retain
                product = retain
                for level, by in enumerate(levels):
                    keep = inside(by, d)
                    steps[d, level, rows, :] = jnp.where(keep, product, 0.0)
                    product = product * jnp.where(keep, shifted(product, by, d), 1.0)
                tails[d, rows, :] = jnp.where(inside(1, d), shifted(product, 1, d), 1.0)
                slopes[d, 3, rows, 0:128] = jnp.broadcast_to(
                    product[:, 0:1] if d == 0 else product[:, length - 1 : length],
                    (block_width, 128),
                )
            value = branch_ref[rows, :].astype(f32)
            scale = 0.7978845608028654
            tanh = jnp.tanh(scale * (value + 0.044715 * value * value * value))
            half = 0.5 * (1.0 + tanh)
            gelu = value * half
            slope = half + 0.5 * value * (1.0 - tanh * tanh) * scale * (
                1.0 + 3.0 * 0.044715 * value * value
            )
            mix[rows, :] = (lru_out * gelu).astype(bf16)
            gelu_val[rows, :] = gelu
            gelu_slope[rows, :] = lru_out * slope

        for load in loads:
            load.wait()

        @pl.loop(0, groups)
        def _(j):
            @pl.when(j < groups - 2)
            def _():
                start_forward(j + 1)

            start_pass(j)

            @pl.when(j > 0)
            def _():
                reduce_near(j - 1)

            end_pass(j)
            compute(j)

            @pl.when(j > 0)
            def _():
                reduce_far(j - 1)

            @pl.when(j == groups - 2)
            def _():
                start_forward(j + 1)

        reduce_near(groups - 1)

        first_contract = (((0,), (0,)), ((), ()))

        @pl.loop(0, full_width // grad_block)
        def _(b):
            cut = pl.ds(pl.multiple_of(b * grad_block, grad_block), grad_block)
            rows = full[:, 0, :, cut].reshape(total_rows, grad_block)
            gate_out[cut, :] = lax.dot_general(
                rows, hid[0], first_contract, preferred_element_type=f32
            ).astype(bf16)
            up_out[cut, :] = lax.dot_general(
                rows, hid[1], first_contract, preferred_element_type=f32
            ).astype(bf16)

        reduce_far(groups - 1)
        rets[me] = ret[me]
        stores = [
            pltpu.make_async_copy(a, b, os.at[i])
            for i, (a, b) in enumerate(
                ((gate_out, gate_hbm), (up_out, up_hbm), (down_out, down_hbm))
            )
        ]
        stores[0].start()
        stores[1].start()

        @pl.loop(0, full_width // grad_block)
        def _(b):
            cut = pl.ds(pl.multiple_of(b * grad_block, grad_block), grad_block)
            grads = full[:, 1, :, cut].reshape(total_rows, grad_block)
            down_out[:, cut] = lax.dot_general(
                act[...], grads, first_contract, preferred_element_type=f32
            ).astype(bf16)

        stores[2].start()

        @pl.loop(1, n)
        def _(k):
            j, i = k // span, k % span
            other = peer(j, i, 1)
            remote(ret.at[other], rets.at[other], bs.at[k], br.at[k], at(sp=other)).wait_recv()

        back = lax.dot_general(
            pick[...], rets[...].reshape(total_rows, width), first_contract,
            preferred_element_type=f32,
        )
        residual = (cot_ref[...].astype(f32) + back).astype(bf16)
        res_ref[...] = residual
        fullres_ref[:, mine] = residual

        def gather_copy(t):
            block = fullres_ref.at[:, mine]
            to = partner if t == 0 else across(t, 1)
            return remote(block, block, gs.at[t], gr.at[t], at(tp=to))

        def gather_pass(t):
            block = fullres_ref.at[:, columns(across(t, -1))]
            return remote(block, block, hs.at[t], hr.at[t], at(tp=partner))

        for t in list(range(1, chips)) + [0]:
            gather_copy(t).start()
        for t in range(1, chips):
            block = fullres_ref.at[:, columns(across(t, -1))]
            remote(block, block, gs.at[t], gr.at[t], at(tp=across(t, -1))).wait_recv()
            gather_pass(t).start()
        block = fullres_ref.at[:, columns(partner)]
        remote(block, block, gs.at[0], gr.at[0], at(tp=partner)).wait_recv()
        for t in range(1, chips):
            block = fullres_ref.at[:, columns(turned(t, -1) * 2 + (1 - core))]
            remote(block, block, hs.at[t], hr.at[t], at(tp=partner)).wait_recv()

        def strip_of(g, i):
            other = g * span + i
            if upright:
                return proj_part.at[:, pl.ds(pl.multiple_of(other * strip, strip), strip)]
            return proj_part.at[pl.ds(pl.multiple_of(other * strip, strip), strip), :]

        def read_strip(other):
            where = pl.ds(pl.multiple_of(other * strip, strip), strip)
            return (proj_part[:, where] if upright else proj_part[where, :]).astype(f32)

        def inner_peer(i, sign):
            return lax.rem(inner + sign * i + span, span)

        def outer_peer(g, sign):
            return lax.rem(group + sign * g + groups, groups)

        def inner_copy(g, i):
            other = outer_peer(g, 1)
            return remote(
                strip_of(other, inner_peer(i, 1)), proj_near.at[g, i], xs.at[g, i], xr.at[g, i],
                at(sp=group * span + inner_peer(i, 1)),
            )

        def outer_copy(g):
            return remote(
                proj_sum.at[g], proj_far.at[g], zs.at[g], zr.at[g],
                at(sp=outer_peer(g, 1) * span + inner),
            )

        turns = list(range(1, groups))
        turns = sorted(turns, key=lambda g: abs(g - groups // 2)) + [0]
        if upright:
            @pl.loop(0, full_width // column_block)
            def _(b):
                cut = pl.ds(pl.multiple_of(b * column_block, column_block), column_block)
                proj_part[:, cut] = jnp.dot(
                    mix[...], fullres_ref[:, cut], preferred_element_type=f32
                ).astype(bf16)
        else:
            @pl.loop(0, full_width // column_block)
            def _(b):
                cut = pl.ds(pl.multiple_of(b * column_block, column_block), column_block)
                proj_part[cut, :] = lax.dot_general(
                    fullres_ref[:, cut], mix[...], (((0,), (1,)), ((), ())),
                    preferred_element_type=f32,
                ).astype(bf16)

        for g in turns:
            for i in range(1, span):
                inner_copy(g, i).start()

        mix_grad[...] = lax.dot_general(
            outp_ref[...], fullres_ref[...], (((1,), (1,)), ((), ())), preferred_element_type=f32
        )
        lane = lax.broadcasted_iota(jnp.int32, (block_width, 128), 1)

        @pl.loop(0, blocks)
        def _(b):
            rows = pl.ds(pl.multiple_of(b * block_width, block_width), block_width)
            upper = mix_grad[rows, :]
            branch_out[rows, :] = upper * gelu_slope[rows, :]
            grad = upper * gelu_val[rows, :]
            last = []
            for d in range(2):
                carried = decay[d, rows, :] * grad
                for level, by in enumerate(levels):
                    carried = carried + steps[d, level, rows, :] * shifted(carried, by, d)
                local[d, rows, :] = grad + jnp.where(inside(1, d), shifted(carried, 1, d), 0.0)
                last.append(carried[:, 0:1] if d == 0 else carried[:, length - 1 : length])
            packed_ends = jnp.where(lane == 0, last[0], jnp.where(lane == 1, last[1], 0.0))
            packed_ends = jnp.where(lane == 2, slopes[0, 3, rows, 0:128], packed_ends)
            ends[rows, :] = jnp.where(lane == 3, slopes[1, 3, rows, 0:128], packed_ends)

        if channels < channels_pad:
            ends[channels:, :] = jnp.zeros((channels_pad - channels, 128), f32)
        ends_row[...] = ends[...].T[0:8, :]

        def ends_copy(k):
            return remote(
                ends_row, ends_all.at[me], es.at[k], er.at[k], at(sp=lax.rem(me + k, n))
            )

        @pl.loop(1, n)
        def _(k):
            ends_copy(k).start()

        ends_all[me] = ends_row[...]

        for g in turns:
            total_strip = read_strip(outer_peer(g, 1) * span + inner)
            for i in range(1, span):
                inner_copy(g, i).wait_recv()
                total_strip = total_strip + proj_near[g, i].astype(f32)
            proj_sum[g] = total_strip.astype(bf16)
            if g > 0:
                outer_copy(g).start()

        @pl.loop(1, n)
        def _(k):
            origin = lax.rem(me - k + n, n)
            remote(
                ends_row, ends_all.at[origin], es.at[k], er.at[k], at(sp=origin)
            ).wait_recv()

        incoming = [jnp.zeros((1, channels_pad), f32)] * 2
        for turn in range(n - 1):
            late = n - 1 - turn
            incoming[0] = jnp.where(
                late > me, ends_all[late, 2:3, :] * incoming[0] + ends_all[late, 0:1, :], incoming[0]
            )
            incoming[1] = jnp.where(
                turn < me, ends_all[turn, 3:4, :] * incoming[1] + ends_all[turn, 1:2, :], incoming[1]
            )
        line = lax.broadcasted_iota(jnp.int32, (128, channels_pad), 0)
        carry[...] = jnp.where(line == 0, incoming[0], jnp.where(line == 1, incoming[1], 0.0)).T

        @pl.loop(0, blocks)
        def _(b):
            rows = pl.ds(pl.multiple_of(b * block_width, block_width), block_width)
            value = jnp.zeros((block_width, length), f32)
            for d in range(2):
                delta = local[d, rows, :] + tails[d, rows, :] * carry[rows, d : d + 1]
                value = value + delta * slopes[d, 2, rows, :]
                value = value + jnp.dot(
                    wr_ref[d, b], (delta * slopes[d, 0, rows, :]).astype(bf16),
                    preferred_element_type=f32,
                )
                value = value + jnp.dot(
                    wi_ref[d, b], (delta * slopes[d, 1, rows, :]).astype(bf16),
                    preferred_element_type=f32,
                )
            conv_out[rows, :] = value

        summed = proj_sum[0].astype(f32)
        for g in turns[:-1]:
            outer_copy(g).wait_recv()
            summed = summed + proj_far[g].astype(f32)
        proj_ref[...] = summed if upright else summed.T

        for g in turns:
            for i in range(1, span):
                inner_copy(g, i).wait_send()
            if g > 0:
                outer_copy(g).wait_send()

        @pl.loop(1, n)
        def _(k):
            ends_copy(k).wait_send()

        @pl.loop(1, n)
        def _(k):
            j, i = k // span, k % span
            dispatch_copy(j, i, 1).wait_send()
            return_copy(j, i).wait_send()

        @pl.loop(0, groups)
        def _(j):
            for i in range(fine):
                for copy in hand_over(j, i):
                    copy.wait_send()
                for t in range(1, chips):
                    pass_on(j, i, t).wait_send()
            for t in range(chips):
                near_copy(j, t).wait_send()
            for t in range(1, chips):
                far_copy(j, t).wait_send()

        for t in range(chips):
            gather_copy(t).wait_send()
        for t in range(1, chips):
            gather_pass(t).wait_send()
        for store in stores:
            store.wait()

    dma = pltpu.SemaphoreType.DMA
    wide = max(chips, 2)
    sem = lambda *shape: [dma(shape)] * 2
    any_spec = pl.BlockSpec(memory_space=pl.ANY)
    shape = jax.ShapeDtypeStruct
    strip_shape = (channels, strip) if upright else (strip, channels)
    part_shape = (channels, full_width) if upright else (full_width, channels)
    return pl.pallas_call(
        kernel, name="layer_backward",
        out_shape=(
            shape((tokens, width), bf16), shape((channels, strip), f32),
            shape((channels, length), f32), shape((channels, length), f32),
            shape(w_gate.shape, bf16), shape(w_up.shape, bf16), shape(w_down.shape, bf16),
        ),
        in_specs=[VMEM_SPEC] * 13 + [any_spec] * 3,
        out_specs=(VMEM_SPEC,) * 4 + (any_spec,) * 3,
        scratch_shapes=[
            pltpu.VMEM(w_gate.shape, bf16), pltpu.VMEM(w_up.shape, bf16), pltpu.VMEM(w_down.shape, bf16),
            pltpu.VMEM((128, tokens), f32), pltpu.VMEM((128, tokens), f32),
            pltpu.VMEM((total_rows, tokens), bf16),
            pltpu.VMEM((n, 2, cap, width), bf16),
            pltpu.VMEM((n, 2, cap, full_width), bf16),
            pltpu.VMEM((2, total_rows, hidden), bf16),
            pltpu.VMEM((total_rows, hidden), bf16),
            pltpu.VMEM((total_rows, full_width), bf16),
            pltpu.VMEM((groups, chips, chunk, width), bf16),
            pltpu.VMEM((groups, chips, chunk, width), bf16),
            pltpu.VMEM((groups, chips, chunk, width), bf16),
            pltpu.VMEM((n, cap, width), bf16), pltpu.VMEM((n, cap, width), bf16),
            pltpu.VMEM(w_gate.shape, bf16), pltpu.VMEM(w_up.shape, bf16), pltpu.VMEM(w_down.shape, bf16),
            pltpu.VMEM((tokens, full_width), bf16),
            pltpu.VMEM((2, 4, channels, length), f32),
            pltpu.VMEM((2, len(levels), channels, length), f32),
            pltpu.VMEM((2, channels, length), f32), pltpu.VMEM((2, channels, length), f32),
            pltpu.VMEM((2, channels, 128), f32),
            pltpu.VMEM((channels, length), bf16),
            pltpu.VMEM((channels, length), f32), pltpu.VMEM((channels, length), f32),
            pltpu.VMEM((channels, length), f32), pltpu.VMEM((2, channels, length), f32),
            pltpu.VMEM((channels_pad, 128), f32), pltpu.VMEM((8, channels_pad), f32),
            pltpu.VMEM((n, 8, channels_pad), f32), pltpu.VMEM((channels_pad, 128), f32),
            pltpu.VMEM(part_shape, bf16),
            pltpu.VMEM((groups, span) + strip_shape, bf16),
            pltpu.VMEM((groups,) + strip_shape, bf16), pltpu.VMEM((groups,) + strip_shape, bf16),
        ]
        + sem(n) + sem(groups, span) + sem(groups)
        + [dma((3,))]
        + sem(n) + sem(units, wide) + sem(units) + sem(units, wide)
        + sem(groups, wide) + sem(groups, wide) + sem(n) + sem(wide) + sem(wide) + [dma((3,))],
        compiler_params=pltpu.CompilerParams(
            collective_id=1, has_side_effects=True, vmem_limit_bytes=60 * 1024 * 1024
        ),
    )(
        cotangent, moe_input, routes, gates, conv_in, branch, state_before, state_after, jump,
        recur_weight, input_weight, lam, out_proj, w_gate, w_up, w_down,
    )


def on_device(
    cotangent, moe_input, routes, gates, w_gate, w_up, w_down, out_proj, conv_in, branch,
    state_before, state_after, jump, recur_weight, input_weight, lam,
):
    residual_grad, out_proj_grad, conv_grad, branch_grad, gate_grad, up_grad, down_grad = (
        layer_backward(
            cotangent, moe_input, routes, gates, w_gate[0], w_up[0], w_down[0], out_proj, conv_in,
            branch, state_before, state_after, jump, recur_weight, input_weight, lam,
        )
    )
    return (
        gate_grad[None], up_grad[None], down_grad[None],
        residual_grad, out_proj_grad, conv_grad, branch_grad,
    )


def solution(mesh):
    placed = (
        P("sp", "tp"),
        P("sp", "tp"),
        P("sp", None),
        P("sp", None),
        P("sp", None, "tp"),
        P("sp", None, "tp"),
        P("sp", "tp", None),
        P("tp", None),
        P("tp", "sp"),
        P("tp", "sp"),
        P("tp", "sp"),
        P("tp", "sp"),
        P("tp", "sp"),
        P(None, "tp", None, None),
        P(None, "tp", None, None),
        P(None, "tp"),
    )
    return jax.shard_map(
        on_device,
        mesh=mesh,
        in_specs=placed,
        out_specs=(
            P("sp", None, "tp"),
            P("sp", None, "tp"),
            P("sp", "tp", None),
            P("sp", "tp"),
            P("tp", "sp"),
            P("tp", "sp"),
            P("tp", "sp"),
        ),
        check_vma=False,
    )
```

```python
import jax
import jax.numpy as jnp
from jax import lax
from jax.experimental import pallas as pl
from jax.experimental.pallas import tpu as pltpu
from jax.sharding import PartitionSpec as P

decay_scale = 8.0


MESH = pl.DeviceIdType.MESH
VMEM_SPEC = pl.BlockSpec(memory_space=pltpu.VMEM)


def at(sp=None, tp=None):
    sp = lax.axis_index("sp") if sp is None else sp
    tp = lax.axis_index("tp") if tp is None else tp
    return (sp, tp)


def meet(devices):
    barrier = pltpu.get_barrier_semaphore()
    for device in devices:
        pl.semaphore_signal(barrier, inc=1, device_id=device, device_id_type=MESH)
    pl.semaphore_wait(barrier, len(devices))


def remote(source, target, send, recv, device):
    return pltpu.make_async_remote_copy(
        src_ref=source, dst_ref=target, send_sem=send, recv_sem=recv,
        device_id=device, device_id_type=MESH,
    )


def softplus(value):
    small = jnp.exp(-jnp.abs(value))
    series = small * (1.0 - small * (0.5 - small * (1.0 / 3.0 - small * 0.25)))
    return jnp.maximum(value, 0.0) + jnp.where(small < 0.01, series, jnp.log(1.0 + small))


def one_minus_exp(value, exponential):
    series = -value * (
        1.0 + value * (0.5 + value * (1.0 / 6.0 + value * (1.0 / 24.0 + value * (
            1.0 / 120.0 + value * (1.0 / 720.0)
        ))))
    )
    return jnp.where(value > -0.25, series, 1.0 - exponential)


def layer_backward(
    cotangent, moe_input, routes, gates, w_gate, w_up, w_down, out_proj, conv_in, branch,
    state_before, state_after, jump, recur_weight, input_weight, lam,
):
    n, tp = lax.axis_size("sp"), lax.axis_size("tp")
    chips = tp // 2
    tokens, width = cotangent.shape
    full_width, hidden = w_gate.shape
    cap = -(-(3 * tokens // n) // 16) * 16
    span = min(n, 2 if n <= 8 else 4)
    groups = n // span
    fine = span if n <= 8 else 1
    per_unit = span // fine
    units = groups * fine
    chunk = span * cap
    total_rows = n * cap
    hidden_block = min(hidden, 256)
    column_block = min(full_width, 512)
    grad_block = min(full_width, 256)
    f32, bf16 = jnp.float32, jnp.bfloat16
    channels, length = conv_in.shape
    blocks, block_width = recur_weight.shape[1:3]
    channels_pad = max(channels, 128)
    strip = full_width // n
    upright = strip % 128 == 0
    levels = [1 << i for i in range((length - 1).bit_length())]

    def kernel(
        cot_ref, in_ref, routes_ref, gates_ref, conv_ref, branch_ref, before_ref, after_ref,
        jump_ref, wr_ref, wi_ref, lam_ref, outp_ref, wg_hbm, wu_hbm, wd_hbm,
        res_ref, proj_ref, conv_out, branch_out, gate_out, up_out, down_out,
        wg, wu, wd, key_t, gate_t, pick, send, full, hid, act, part, near, total, far, ret, rets,
        fullres_ref,
        slopes, steps, decay, tails, speed, mix, gelu_val, gelu_slope, mix_grad, local,
        ends, ends_row, ends_all, carry, proj_part, proj_near, proj_sum, proj_far,
        es, er, xs, xr, zs, zr,
        ws, ss, sr, ys, yr, ps, pr, fs, fr, ns, nr, ts, tr, bs, br, gs, gr, hs, hr,
    ):
        me, place = lax.axis_index("sp"), lax.axis_index("tp")
        chip, core = place // 2, place % 2
        partner = chip * 2 + (1 - core)
        group, inner = me // span, me % span

        def columns(member):
            return pl.ds(pl.multiple_of(member * width, width), width)

        mine = columns(place)

        def turned(t, sign):
            return lax.rem(chip + sign * t + chips, chips)

        def across(t, sign):
            return turned(t, sign) * 2 + core

        def order(j):
            return jnp.where(j < 2, j, groups + 1 - j)

        def group_of(j, sign):
            return lax.rem(group + sign * order(j) + groups, groups)

        def peer(j, i, sign):
            return group_of(j, sign) * span + lax.rem(inner + sign * i + span, span)

        weights = ((wg_hbm, wg), (wu_hbm, wu), (wd_hbm, wd))
        loads = [pltpu.make_async_copy(a, b, ws.at[i]) for i, (a, b) in enumerate(weights)]
        for load in loads:
            load.start()

        meet(
            [at(sp=lax.rem(me + k, n)) for k in range(1, n)]
            + [at(tp=partner)]
            + [at(tp=across(t, 1)) for t in range(1, chips)]
        )

        expert_id = lax.broadcasted_iota(jnp.int32, (128, tokens), 0)
        first = expert_id == routes_ref[0:1, :]
        second = expert_id == routes_ref[1:2, :]
        member = jnp.where(first | second, 1.0, 0.0).astype(f32)
        gate_t[...] = jnp.where(first, gates_ref[0:1, :], 0.0) + jnp.where(
            second, gates_ref[1:2, :], 0.0
        )
        earlier = lax.broadcasted_iota(jnp.int32, (tokens, tokens), 0) < lax.broadcasted_iota(
            jnp.int32, (tokens, tokens), 1
        )
        earlier = jnp.where(earlier, 1.0, 0.0).astype(bf16)
        position = jnp.dot(member.astype(bf16), earlier, preferred_element_type=f32)
        key_t[...] = jnp.where(member > 0.5, position, -1.0)
        row_id = lax.broadcasted_iota(jnp.int32, (cap, tokens), 0).astype(f32)

        def packed(to):
            chosen = row_id == key_t[pl.ds(to, 1), :]
            one_hot = jnp.where(chosen, 1.0, 0.0).astype(bf16)
            scale = jnp.sum(jnp.where(chosen, gate_t[pl.ds(to, 1), :], 0.0), axis=1, keepdims=True)
            pick[pl.ds(pl.multiple_of(to * cap, 16), cap), :] = one_hot
            rows = jnp.dot(one_hot, in_ref[...], preferred_element_type=f32).astype(bf16)
            grads = jnp.dot(one_hot, cot_ref[...], preferred_element_type=f32) * scale
            return rows, grads.astype(bf16)

        rows, grads = packed(me)
        full[me, 0, :, mine] = rows
        full[me, 1, :, mine] = grads

        def unit_slice(j, i):
            base = group_of(j, -1) * span
            if fine > 1:
                return pl.ds(base + lax.rem(inner - i + span, span), 1)
            return pl.ds(base, span)

        def dispatch_copy(j, i, sign):
            other = peer(j, i, sign)
            k = j * span + i
            return remote(
                send.at[other], full.at[me if sign > 0 else other, :, :, mine],
                ss.at[k], sr.at[k], at(sp=other),
            )

        def hand_over(j, i):
            block = full.at[unit_slice(j, i), :, :, mine]
            u = j * fine + i
            out = [
                remote(block, block, ys.at[u, t], yr.at[u, t], at(tp=across(t, 1)))
                for t in range(1, chips)
            ]
            out.append(remote(block, block, ps.at[u], pr.at[u], at(tp=partner)))
            return out

        def pass_on(j, i, t):
            block = full.at[unit_slice(j, i), :, :, columns(across(t, -1))]
            u = j * fine + i
            return remote(block, block, fs.at[u, t], fr.at[u, t], at(tp=partner))

        def start_forward(j, begin=0, end=fine):
            for i in range(begin, min(end, fine)):
                for s in range(per_unit):
                    number = i * per_unit + s

                    @pl.when(j * span + number > 0)
                    def _():
                        dispatch_copy(j, number, -1).wait_recv()

                for copy in hand_over(j, i):
                    copy.start()

        half = span // 2

        def release(j, begin, end):
            @pl.when(j < groups)
            def _():
                for i in range(begin, end):
                    dispatch_copy(j, i, 1).start()

        def start_pass(j):
            for i in range(fine):
                u = j * fine + i
                for t in range(1, chips):
                    block = full.at[unit_slice(j, i), :, :, columns(across(t, -1))]
                    remote(
                        block, block, ys.at[u, t], yr.at[u, t], at(tp=across(t, -1))
                    ).wait_recv()
                    pass_on(j, i, t).start()

        def end_pass(j):
            for i in range(fine):
                u = j * fine + i
                block = full.at[unit_slice(j, i), :, :, columns(partner)]
                remote(block, block, ps.at[u], pr.at[u], at(tp=partner)).wait_recv()
                for t in range(1, chips):
                    block = full.at[
                        unit_slice(j, i), :, :, columns(turned(t, -1) * 2 + (1 - core))
                    ]
                    remote(block, block, fs.at[u, t], fr.at[u, t], at(tp=partner)).wait_recv()

        def chunk_rows(j):
            return pl.ds(pl.multiple_of(group_of(j, -1) * chunk, 16), chunk)

        def near_copy(j, t):
            return remote(
                part.at[chunk_rows(j), columns(turned(t, 1) * 2 + (1 - core))],
                near.at[j, t], ns.at[j, t], nr.at[j, t], at(tp=partner),
            )

        def far_copy(j, t):
            return remote(
                total.at[j, t], far.at[j, t], ts.at[j, t], tr.at[j, t], at(tp=across(t, 1))
            )

        def compute(j):
            base = group_of(j, -1) * span
            where = chunk_rows(j)

            @pl.loop(0, hidden // hidden_block)
            def _(b):
                cut = pl.ds(pl.multiple_of(b * hidden_block, hidden_block), hidden_block)
                rows = full[pl.ds(base, span), 0].reshape(chunk, full_width)
                pre_gate = jnp.dot(rows, wg[:, cut], preferred_element_type=f32)
                pre_up = jnp.dot(rows, wu[:, cut], preferred_element_type=f32)
                grads = full[pl.ds(base, span), 1].reshape(chunk, full_width)
                act_grad = lax.dot_general(
                    grads, wd[cut, :], (((1,), (1,)), ((), ())), preferred_element_type=f32
                )
                sigmoid = jax.nn.sigmoid(pre_gate)
                silu = pre_gate * sigmoid
                slope = sigmoid * (1.0 + pre_gate * (1.0 - sigmoid))
                act[where, cut] = (silu * pre_up).astype(bf16)
                hid[0, where, cut] = (act_grad * pre_up * slope).astype(bf16)
                hid[1, where, cut] = (act_grad * silu).astype(bf16)

            @pl.loop(0, full_width // column_block)
            def _(b):
                cut = pl.ds(pl.multiple_of(b * column_block, column_block), column_block)
                value = lax.dot_general(
                    hid[0, where, :], wg[cut, :], (((1,), (1,)), ((), ())), preferred_element_type=f32
                ) + lax.dot_general(
                    hid[1, where, :], wu[cut, :], (((1,), (1,)), ((), ())), preferred_element_type=f32
                )
                part[where, cut] = value.astype(bf16)

            for t in range(chips):
                near_copy(j, t).start()

        def reduce_near(j):
            where = chunk_rows(j)
            for t in list(range(1, chips)) + [0]:
                near_copy(j, t).wait_recv()
                if t > 0:
                    value = part[where, columns(turned(t, 1) * 2 + core)].astype(f32) + near[
                        j, t
                    ].astype(f32)
                    total[j, t] = value.astype(bf16)
                    far_copy(j, t).start()

        def return_copy(j, i):
            other = peer(j, i, -1)
            k = j * span + i
            return remote(ret.at[other], rets.at[me], bs.at[k], br.at[k], at(sp=other))

        def reduce_far(j):
            where = chunk_rows(j)
            value = part[where, mine].astype(f32) + near[j, 0].astype(f32)
            for t in range(1, chips):
                far_copy(j, t).wait_recv()
                value = value + far[j, t].astype(f32)
            ret[pl.ds(group_of(j, -1) * span, span)] = value.astype(bf16).reshape(span, cap, width)
            for i in range(span):

                @pl.when(j * span + i > 0)
                def _():
                    return_copy(j, i).start()

        if fine > 1:
            for copy in hand_over(0, 0):
                copy.start()

        @pl.loop(1, n)
        def _(k):
            j, i = k // span, k % span
            to = peer(j, i, 1)
            rows, grads = packed(to)
            send[to, 0] = rows
            send[to, 1] = grads

            @pl.when(j < 2)
            def _():
                dispatch_copy(j, i, 1).start()

        start_forward(0, 1 if fine > 1 else 0)
        release(2, 0, span)

        diagonal = lax.broadcasted_iota(jnp.int32, (channels, channels), 0) == (
            lax.broadcasted_iota(jnp.int32, (channels, channels), 1)
        )
        for d in range(2):
            column = jnp.sum(
                jnp.where(diagonal, lam_ref[d : d + 1, :], 0.0), axis=1, keepdims=True
            )
            speed[d] = decay_scale * softplus(-jnp.broadcast_to(column, (channels, 128)))
        token = lax.broadcasted_iota(jnp.int32, (block_width, length), 1)

        def shifted(value, by, d):
            return pltpu.roll(value, length - by if d == 0 else by, 1)

        def inside(by, d):
            return token < length - by if d == 0 else token >= by

        @pl.loop(0, blocks)
        def _(b):
            rows = pl.ds(pl.multiple_of(b * block_width, block_width), block_width)
            conv = conv_ref[rows, :]
            wide = conv.astype(f32)
            lru_out = jnp.zeros((block_width, length), f32)
            for d, state_ref in enumerate((before_ref, after_ref)):
                recur = jax.nn.sigmoid(
                    lax.dot_general(
                        wr_ref[d, b], conv, (((0,), (0,)), ((), ())), preferred_element_type=f32
                    )
                )
                inward = jax.nn.sigmoid(
                    lax.dot_general(
                        wi_ref[d, b], conv, (((0,), (0,)), ((), ())), preferred_element_type=f32
                    )
                )
                rate = speed[d, rows, 0:1]
                log_decay = jump_ref[rows, :] - rate * recur
                retain = jnp.exp(log_decay)
                root = jnp.sqrt(one_minus_exp(2.0 * log_decay, retain * retain))
                state = state_ref[rows, :]
                lru_out = lru_out + retain * state + root * inward * wide
                log_slope = state * retain - inward * wide * retain * retain / root
                slopes[d, 0, rows, :] = -rate * log_slope * recur * (1.0 - recur)
                slopes[d, 1, rows, :] = root * wide * inward * (1.0 - inward)
                slopes[d, 2, rows, :] = root * inward
                decay[d, rows, :] = retain
                product = retain
                for level, by in enumerate(levels):
                    keep = inside(by, d)
                    steps[d, level, rows, :] = jnp.where(keep, product, 0.0)
                    product = product * jnp.where(keep, shifted(product, by, d), 1.0)
                tails[d, rows, :] = jnp.where(inside(1, d), shifted(product, 1, d), 1.0)
                slopes[d, 3, rows, 0:128] = jnp.broadcast_to(
                    product[:, 0:1] if d == 0 else product[:, length - 1 : length],
                    (block_width, 128),
                )
            value = branch_ref[rows, :].astype(f32)
            scale = 0.7978845608028654
            tanh = jnp.tanh(scale * (value + 0.044715 * value * value * value))
            half = 0.5 * (1.0 + tanh)
            gelu = value * half
            slope = half + 0.5 * value * (1.0 - tanh * tanh) * scale * (
                1.0 + 3.0 * 0.044715 * value * value
            )
            mix[rows, :] = (lru_out * gelu).astype(bf16)
            gelu_val[rows, :] = gelu
            gelu_slope[rows, :] = lru_out * slope

        for load in loads:
            load.wait()

        @pl.loop(0, groups)
        def _(j):
            @pl.when(j < groups - 2)
            def _():
                start_forward(j + 1)
                release(j + 3, 0, half)

            @pl.when((j > 0) & (j < groups - 2))
            def _():
                release(j + 2, half, span)

            start_pass(j)
            end_pass(j)
            compute(j)

            @pl.when(j == groups - 2)
            def _():
                start_forward(groups - 1, 1)

            @pl.when((j > 0) & (j < groups - 1))
            def _():
                reduce_near(j)

            @pl.when(j == groups - 3)
            def _():
                start_forward(groups - 1, 0, 1)

            @pl.when(j > 1)
            def _():
                reduce_far(j - 1)

        reduce_near(groups - 1)
        reduce_near(0)
        first_contract = (((0,), (0,)), ((), ()))

        @pl.loop(0, full_width // grad_block)
        def _(b):
            cut = pl.ds(pl.multiple_of(b * grad_block, grad_block), grad_block)
            rows = full[:, 0, :, cut].reshape(total_rows, grad_block)
            gate_out[cut, :] = lax.dot_general(
                rows, hid[0], first_contract, preferred_element_type=f32
            ).astype(bf16)
            up_out[cut, :] = lax.dot_general(
                rows, hid[1], first_contract, preferred_element_type=f32
            ).astype(bf16)

        reduce_far(groups - 1)
        @pl.loop(0, full_width // grad_block)
        def _(b):
            cut = pl.ds(pl.multiple_of(b * grad_block, grad_block), grad_block)
            grads = full[:, 1, :, cut].reshape(total_rows, grad_block)
            down_out[:, cut] = lax.dot_general(
                act[...], grads, first_contract, preferred_element_type=f32
            ).astype(bf16)

        reduce_far(0)
        rets[me] = ret[me]

        @pl.loop(1, n)
        def _(k):
            j, i = k // span, k % span
            other = peer(j, i, 1)
            remote(ret.at[other], rets.at[other], bs.at[k], br.at[k], at(sp=other)).wait_recv()

        back = lax.dot_general(
            pick[...], rets[...].reshape(total_rows, width), first_contract,
            preferred_element_type=f32,
        )
        residual = (cot_ref[...].astype(f32) + back).astype(bf16)
        res_ref[...] = residual
        fullres_ref[:, mine] = residual

        def gather_copy(t):
            block = fullres_ref.at[:, mine]
            to = partner if t == 0 else across(t, 1)
            return remote(block, block, gs.at[t], gr.at[t], at(tp=to))

        def gather_pass(t):
            block = fullres_ref.at[:, columns(across(t, -1))]
            return remote(block, block, hs.at[t], hr.at[t], at(tp=partner))

        for t in list(range(1, chips)) + [0]:
            gather_copy(t).start()
        for t in range(1, chips):
            block = fullres_ref.at[:, columns(across(t, -1))]
            remote(block, block, gs.at[t], gr.at[t], at(tp=across(t, -1))).wait_recv()
            gather_pass(t).start()
        block = fullres_ref.at[:, columns(partner)]
        remote(block, block, gs.at[0], gr.at[0], at(tp=partner)).wait_recv()
        for t in range(1, chips):
            block = fullres_ref.at[:, columns(turned(t, -1) * 2 + (1 - core))]
            remote(block, block, hs.at[t], hr.at[t], at(tp=partner)).wait_recv()

        def strip_of(g, i):
            other = g * span + i
            if upright:
                return proj_part.at[:, pl.ds(pl.multiple_of(other * strip, strip), strip)]
            return proj_part.at[pl.ds(pl.multiple_of(other * strip, strip), strip), :]

        def read_strip(other):
            where = pl.ds(pl.multiple_of(other * strip, strip), strip)
            return (proj_part[:, where] if upright else proj_part[where, :]).astype(f32)

        def inner_peer(i, sign):
            return lax.rem(inner + sign * i + span, span)

        def outer_peer(g, sign):
            return lax.rem(group + sign * g + groups, groups)

        def inner_copy(g, i):
            other = outer_peer(g, 1)
            return remote(
                strip_of(other, inner_peer(i, 1)), proj_near.at[g, i], xs.at[g, i], xr.at[g, i],
                at(sp=group * span + inner_peer(i, 1)),
            )

        def outer_copy(g):
            return remote(
                proj_sum.at[g], proj_far.at[g], zs.at[g], zr.at[g],
                at(sp=outer_peer(g, 1) * span + inner),
            )

        turns = list(range(1, groups))
        turns = sorted(turns, key=lambda g: abs(g - groups // 2)) + [0]
        turn_width = span * strip

        def project(g):
            where = pl.ds(pl.multiple_of(outer_peer(g, 1) * turn_width, turn_width), turn_width)
            if upright:
                proj_part[:, where] = jnp.dot(
                    mix[...], fullres_ref[:, where], preferred_element_type=f32
                ).astype(bf16)
            else:
                proj_part[where, :] = lax.dot_general(
                    fullres_ref[:, where], mix[...], (((0,), (1,)), ((), ())),
                    preferred_element_type=f32,
                ).astype(bf16)
            for i in range(1, span):
                inner_copy(g, i).start()

        def finish_inner(g):
            total_strip = read_strip(outer_peer(g, 1) * span + inner)
            for i in range(1, span):
                inner_copy(g, i).wait_recv()
                total_strip = total_strip + proj_near[g, i].astype(f32)
            proj_sum[g] = total_strip.astype(bf16)
            if g > 0:
                outer_copy(g).start()

        project(turns[0])
        mix_grad[...] = lax.dot_general(
            outp_ref[...], fullres_ref[...], (((1,), (1,)), ((), ())), preferred_element_type=f32
        )
        lane = lax.broadcasted_iota(jnp.int32, (block_width, 128), 1)

        @pl.loop(0, blocks)
        def _(b):
            rows = pl.ds(pl.multiple_of(b * block_width, block_width), block_width)
            upper = mix_grad[rows, :]
            branch_out[rows, :] = upper * gelu_slope[rows, :]
            grad = upper * gelu_val[rows, :]
            last = []
            for d in range(2):
                carried = decay[d, rows, :] * grad
                for level, by in enumerate(levels):
                    carried = carried + steps[d, level, rows, :] * shifted(carried, by, d)
                local[d, rows, :] = grad + jnp.where(inside(1, d), shifted(carried, 1, d), 0.0)
                last.append(carried[:, 0:1] if d == 0 else carried[:, length - 1 : length])
            packed_ends = jnp.where(lane == 0, last[0], jnp.where(lane == 1, last[1], 0.0))
            packed_ends = jnp.where(lane == 2, slopes[0, 3, rows, 0:128], packed_ends)
            ends[rows, :] = jnp.where(lane == 3, slopes[1, 3, rows, 0:128], packed_ends)

        if channels < channels_pad:
            ends[channels:, :] = jnp.zeros((channels_pad - channels, 128), f32)
        ends_row[...] = ends[...].T[0:8, :]

        def ends_copy(k):
            return remote(
                ends_row, ends_all.at[me], es.at[k], er.at[k], at(sp=lax.rem(me + k, n))
            )

        @pl.loop(1, n)
        def _(k):
            ends_copy(k).start()

        ends_all[me] = ends_row[...]

        for g in turns[1:]:
            project(g)
        for g in turns[:-2]:
            finish_inner(g)
        @pl.loop(1, n)
        def _(k):
            origin = lax.rem(me - k + n, n)
            remote(
                ends_row, ends_all.at[origin], es.at[k], er.at[k], at(sp=origin)
            ).wait_recv()

        incoming = [jnp.zeros((1, channels_pad), f32)] * 2
        for turn in range(n - 1):
            late = n - 1 - turn
            incoming[0] = jnp.where(
                late > me, ends_all[late, 2:3, :] * incoming[0] + ends_all[late, 0:1, :], incoming[0]
            )
            incoming[1] = jnp.where(
                turn < me, ends_all[turn, 3:4, :] * incoming[1] + ends_all[turn, 1:2, :], incoming[1]
            )
        line = lax.broadcasted_iota(jnp.int32, (128, channels_pad), 0)
        carry[...] = jnp.where(line == 0, incoming[0], jnp.where(line == 1, incoming[1], 0.0)).T

        @pl.loop(0, blocks)
        def _(b):
            rows = pl.ds(pl.multiple_of(b * block_width, block_width), block_width)
            value = jnp.zeros((block_width, length), f32)
            for d in range(2):
                delta = local[d, rows, :] + tails[d, rows, :] * carry[rows, d : d + 1]
                value = value + delta * slopes[d, 2, rows, :]
                value = value + jnp.dot(
                    wr_ref[d, b], (delta * slopes[d, 0, rows, :]).astype(bf16),
                    preferred_element_type=f32,
                )
                value = value + jnp.dot(
                    wi_ref[d, b], (delta * slopes[d, 1, rows, :]).astype(bf16),
                    preferred_element_type=f32,
                )
            conv_out[rows, :] = value

        for g in turns[-2:]:
            finish_inner(g)
        summed = proj_sum[0].astype(f32)
        for g in turns[:-1]:
            outer_copy(g).wait_recv()
            summed = summed + proj_far[g].astype(f32)
        proj_ref[...] = summed if upright else summed.T

        for g in turns:
            for i in range(1, span):
                inner_copy(g, i).wait_send()
            if g > 0:
                outer_copy(g).wait_send()

        @pl.loop(1, n)
        def _(k):
            ends_copy(k).wait_send()

        @pl.loop(1, n)
        def _(k):
            j, i = k // span, k % span
            dispatch_copy(j, i, 1).wait_send()
            return_copy(j, i).wait_send()

        @pl.loop(0, groups)
        def _(j):
            for i in range(fine):
                for copy in hand_over(j, i):
                    copy.wait_send()
                for t in range(1, chips):
                    pass_on(j, i, t).wait_send()
            for t in range(chips):
                near_copy(j, t).wait_send()
            for t in range(1, chips):
                far_copy(j, t).wait_send()

        for t in range(chips):
            gather_copy(t).wait_send()
        for t in range(1, chips):
            gather_pass(t).wait_send()


    dma = pltpu.SemaphoreType.DMA
    wide = max(chips, 2)
    sem = lambda *shape: [dma(shape)] * 2
    any_spec = pl.BlockSpec(memory_space=pl.ANY)
    shape = jax.ShapeDtypeStruct
    strip_shape = (channels, strip) if upright else (strip, channels)
    part_shape = (channels, full_width) if upright else (full_width, channels)
    return pl.pallas_call(
        kernel, name="layer_backward",
        out_shape=(
            pltpu.VMEM((tokens, width), bf16), pltpu.VMEM((channels, strip), f32),
            pltpu.VMEM((channels, length), f32), pltpu.VMEM((channels, length), f32),
            pltpu.VMEM(w_gate.shape, bf16), pltpu.VMEM(w_up.shape, bf16), pltpu.VMEM(w_down.shape, bf16),
        ),
        in_specs=[VMEM_SPEC] * 13 + [any_spec] * 3,
        out_specs=(VMEM_SPEC,) * 7,
        scratch_shapes=[
            pltpu.VMEM(w_gate.shape, bf16), pltpu.VMEM(w_up.shape, bf16), pltpu.VMEM(w_down.shape, bf16),
            pltpu.VMEM((128, tokens), f32), pltpu.VMEM((128, tokens), f32),
            pltpu.VMEM((total_rows, tokens), bf16),
            pltpu.VMEM((n, 2, cap, width), bf16),
            pltpu.VMEM((n, 2, cap, full_width), bf16),
            pltpu.VMEM((2, total_rows, hidden), bf16),
            pltpu.VMEM((total_rows, hidden), bf16),
            pltpu.VMEM((total_rows, full_width), bf16),
            pltpu.VMEM((groups, chips, chunk, width), bf16),
            pltpu.VMEM((groups, chips, chunk, width), bf16),
            pltpu.VMEM((groups, chips, chunk, width), bf16),
            pltpu.VMEM((n, cap, width), bf16), pltpu.VMEM((n, cap, width), bf16),
            pltpu.VMEM((tokens, full_width), bf16),
            pltpu.VMEM((2, 4, channels, length), f32),
            pltpu.VMEM((2, len(levels), channels, length), f32),
            pltpu.VMEM((2, channels, length), f32), pltpu.VMEM((2, channels, length), f32),
            pltpu.VMEM((2, channels, 128), f32),
            pltpu.VMEM((channels, length), bf16),
            pltpu.VMEM((channels, length), f32), pltpu.VMEM((channels, length), f32),
            pltpu.VMEM((channels, length), f32), pltpu.VMEM((2, channels, length), f32),
            pltpu.VMEM((channels_pad, 128), f32), pltpu.VMEM((8, channels_pad), f32),
            pltpu.VMEM((n, 8, channels_pad), f32), pltpu.VMEM((channels_pad, 128), f32),
            pltpu.VMEM(part_shape, bf16),
            pltpu.VMEM((groups, span) + strip_shape, bf16),
            pltpu.VMEM((groups,) + strip_shape, bf16), pltpu.VMEM((groups,) + strip_shape, bf16),
        ]
        + sem(n) + sem(groups, span) + sem(groups)
        + [dma((3,))]
        + sem(n) + sem(units, wide) + sem(units) + sem(units, wide)
        + sem(groups, wide) + sem(groups, wide) + sem(n) + sem(wide) + sem(wide),
        compiler_params=pltpu.CompilerParams(
            collective_id=1, has_side_effects=True, vmem_limit_bytes=54 * 1024 * 1024
        ),
    )(
        cotangent, moe_input, routes.T, gates.T, conv_in, branch, state_before, state_after, jump,
        recur_weight, input_weight, lam, out_proj, w_gate, w_up, w_down,
    )


def write_out(values):
    count = len(values)

    def kernel(*refs):
        sems = refs[2 * count]
        copies = [
            pltpu.make_async_copy(refs[i], refs[count + i], sems.at[i]) for i in range(count)
        ]
        for copy in copies:
            copy.start()
        for copy in copies:
            copy.wait()

    return pl.pallas_call(
        kernel, name="write_out",
        out_shape=tuple(jax.ShapeDtypeStruct(v.shape, v.dtype) for v in values),
        in_specs=[pl.BlockSpec(memory_space=pl.ANY)] * count,
        out_specs=(pl.BlockSpec(memory_space=pl.ANY),) * count,
        scratch_shapes=[pltpu.SemaphoreType.DMA((count,))],
        compiler_params=pltpu.CompilerParams(vmem_limit_bytes=4 * 1024 * 1024),
    )(*values)


def on_device(
    cotangent, moe_input, routes, gates, w_gate, w_up, w_down, out_proj, conv_in, branch,
    state_before, state_after, jump, recur_weight, input_weight, lam,
):
    residual_grad, out_proj_grad, conv_grad, branch_grad, gate_grad, up_grad, down_grad = (
        write_out(layer_backward(
            cotangent, moe_input, routes, gates, w_gate[0], w_up[0], w_down[0], out_proj, conv_in,
            branch, state_before, state_after, jump, recur_weight, input_weight, lam,
        ))
    )
    return (
        gate_grad[None], up_grad[None], down_grad[None],
        residual_grad, out_proj_grad, conv_grad, branch_grad,
    )


def solution(mesh):
    placed = (
        P("sp", "tp"),
        P("sp", "tp"),
        P("sp", None),
        P("sp", None),
        P("sp", None, "tp"),
        P("sp", None, "tp"),
        P("sp", "tp", None),
        P("tp", None),
        P("tp", "sp"),
        P("tp", "sp"),
        P("tp", "sp"),
        P("tp", "sp"),
        P("tp", "sp"),
        P(None, "tp", None, None),
        P(None, "tp", None, None),
        P(None, "tp"),
    )
    return jax.shard_map(
        on_device,
        mesh=mesh,
        in_specs=placed,
        out_specs=(
            P("sp", None, "tp"),
            P("sp", None, "tp"),
            P("sp", "tp", None),
            P("sp", "tp"),
            P("tp", "sp"),
            P("tp", "sp"),
            P("tp", "sp"),
        ),
        check_vma=False,
    )
```

```python
import jax
import jax.numpy as jnp
from jax import lax
from jax.experimental import pallas as pl
from jax.experimental.pallas import tpu as pltpu
from jax.sharding import PartitionSpec as P

decay_scale = 8.0


MESH = pl.DeviceIdType.MESH
VMEM_SPEC = pl.BlockSpec(memory_space=pltpu.VMEM)


def at(sp=None, tp=None):
    sp = lax.axis_index("sp") if sp is None else sp
    tp = lax.axis_index("tp") if tp is None else tp
    return (sp, tp)


def meet(devices):
    barrier = pltpu.get_barrier_semaphore()
    for device in devices:
        pl.semaphore_signal(barrier, inc=1, device_id=device, device_id_type=MESH)
    pl.semaphore_wait(barrier, len(devices))


def remote(source, target, send, recv, device):
    return pltpu.make_async_remote_copy(
        src_ref=source, dst_ref=target, send_sem=send, recv_sem=recv,
        device_id=device, device_id_type=MESH,
    )


def softplus(value):
    small = jnp.exp(-jnp.abs(value))
    series = small * (1.0 - small * (0.5 - small * (1.0 / 3.0 - small * 0.25)))
    return jnp.maximum(value, 0.0) + jnp.where(small < 0.01, series, jnp.log(1.0 + small))


def one_minus_exp(value, exponential):
    series = -value * (
        1.0 + value * (0.5 + value * (1.0 / 6.0 + value * (1.0 / 24.0 + value * (
            1.0 / 120.0 + value * (1.0 / 720.0)
        ))))
    )
    return jnp.where(value > -0.25, series, 1.0 - exponential)


def layer_backward(
    cotangent, moe_input, routes, gates, w_gate, w_up, w_down, out_proj, conv_in, branch,
    state_before, state_after, jump, recur_weight, input_weight, lam,
):
    n, tp = lax.axis_size("sp"), lax.axis_size("tp")
    chips = tp // 2
    tokens, width = cotangent.shape
    full_width, hidden = w_gate.shape
    cap = -(-(3 * tokens // n) // 16) * 16
    span = min(n, 2 if n <= 8 else 4)
    groups = n // span
    fine = span if n <= 8 else 1
    per_unit = span // fine
    units = groups * fine
    chunk = span * cap
    total_rows = n * cap
    pieces = 2 if span % 2 == 0 else 1
    piece_rows, piece_sources = chunk // pieces, span // pieces
    split_last = fine == 2 and pieces == 2
    hidden_block = min(hidden, 256)
    column_block = min(full_width, 512)
    grad_block = min(full_width, 256)
    f32, bf16 = jnp.float32, jnp.bfloat16
    channels, length = conv_in.shape
    blocks, block_width = recur_weight.shape[1:3]
    channels_pad = max(channels, 128)
    strip = full_width // n
    upright = strip % 128 == 0
    halves = 2 if span == 2 and chips == 2 and groups == tp and upright else 1
    half_width = width // halves
    levels = [1 << i for i in range((length - 1).bit_length())]

    def kernel(
        cot_ref, in_ref, routes_ref, gates_ref, conv_ref, branch_ref, before_ref, after_ref,
        jump_ref, wr_ref, wi_ref, lam_ref, outp_ref, wg_hbm, wu_hbm, wd_hbm,
        res_ref, proj_ref, conv_out, branch_out, gate_out, up_out, down_out,
        wg, wu, wd, key_t, gate_t, pick, send, full, hid, act, part, near, total, far, ret, rets,
        fullres_ref,
        slopes, steps, decay, tails, speed, mix_ref, gelu_val, gelu_slope, mix_grad, local,
        ends, ends_row, ends_all, carry, proj_part, proj_near, proj_sum, proj_far,
        es, er, xs, xr, zs, zr,
        ws, ss, sr, ys, yr, ps, pr, fs, fr, ns, nr, ts, tr, bs, br, gs, gr, hs, hr,
    ):
        me, place = lax.axis_index("sp"), lax.axis_index("tp")
        chip, core = place // 2, place % 2
        partner = chip * 2 + (1 - core)
        group, inner = me // span, me % span

        def columns(member):
            return pl.ds(pl.multiple_of(member * width, width), width)

        mine = columns(place)

        def turned(t, sign):
            return lax.rem(chip + sign * t + chips, chips)

        def across(t, sign):
            return turned(t, sign) * 2 + core

        def order(j):
            return jnp.where(j < 2, j, groups + 1 - j)

        def group_of(j, sign):
            return lax.rem(group + sign * order(j) + groups, groups)

        def peer(j, i, sign):
            return group_of(j, sign) * span + lax.rem(inner + sign * i + span, span)

        weights = ((wg_hbm, wg), (wu_hbm, wu), (wd_hbm, wd))
        loads = [pltpu.make_async_copy(a, b, ws.at[i]) for i, (a, b) in enumerate(weights)]
        for load in loads:
            load.start()

        meet(
            [at(sp=lax.rem(me + k, n)) for k in range(1, n)]
            + [at(tp=partner)]
            + [at(tp=across(t, 1)) for t in range(1, chips)]
        )

        expert_id = lax.broadcasted_iota(jnp.int32, (128, tokens), 0)
        first = expert_id == routes_ref[0:1, :]
        second = expert_id == routes_ref[1:2, :]
        member = jnp.where(first | second, 1.0, 0.0).astype(f32)
        gate_t[...] = jnp.where(first, gates_ref[0:1, :], 0.0) + jnp.where(
            second, gates_ref[1:2, :], 0.0
        )
        earlier = lax.broadcasted_iota(jnp.int32, (tokens, tokens), 0) < lax.broadcasted_iota(
            jnp.int32, (tokens, tokens), 1
        )
        earlier = jnp.where(earlier, 1.0, 0.0).astype(bf16)
        position = jnp.dot(member.astype(bf16), earlier, preferred_element_type=f32)
        key_t[...] = jnp.where(member > 0.5, position, -1.0)
        row_id = lax.broadcasted_iota(jnp.int32, (cap, tokens), 0).astype(f32)

        def packed(to):
            chosen = row_id == key_t[pl.ds(to, 1), :]
            one_hot = jnp.where(chosen, 1.0, 0.0).astype(bf16)
            scale = jnp.sum(jnp.where(chosen, gate_t[pl.ds(to, 1), :], 0.0), axis=1, keepdims=True)
            pick[pl.ds(pl.multiple_of(to * cap, 16), cap), :] = one_hot
            rows = jnp.dot(one_hot, in_ref[...], preferred_element_type=f32).astype(bf16)
            grads = jnp.dot(one_hot, cot_ref[...], preferred_element_type=f32) * scale
            return rows, grads.astype(bf16)

        rows, grads = packed(me)
        full[me, 0, :, mine] = rows
        full[me, 1, :, mine] = grads

        def unit_slice(j, i):
            base = group_of(j, -1) * span
            if fine > 1:
                return pl.ds(base + lax.rem(inner - i + span, span), 1)
            return pl.ds(base, span)

        def dispatch_copy(j, i, sign):
            other = peer(j, i, sign)
            k = j * span + i
            return remote(
                send.at[other], full.at[me if sign > 0 else other, :, :, mine],
                ss.at[k], sr.at[k], at(sp=other),
            )

        def hand_over(j, i):
            block = full.at[unit_slice(j, i), :, :, mine]
            u = j * fine + i
            out = [
                remote(block, block, ys.at[u, t], yr.at[u, t], at(tp=across(t, 1)))
                for t in range(1, chips)
            ]
            out.append(remote(block, block, ps.at[u], pr.at[u], at(tp=partner)))
            return out

        def pass_on(j, i, t):
            block = full.at[unit_slice(j, i), :, :, columns(across(t, -1))]
            u = j * fine + i
            return remote(block, block, fs.at[u, t], fr.at[u, t], at(tp=partner))

        def start_forward(j, begin=0, end=fine):
            for i in range(begin, min(end, fine)):
                for s in range(per_unit):
                    number = i * per_unit + s

                    @pl.when(j * span + number > 0)
                    def _():
                        dispatch_copy(j, number, -1).wait_recv()

                for copy in hand_over(j, i):
                    copy.start()

        half = span // 2

        def release(j, begin, end):
            @pl.when(j < groups)
            def _():
                for i in range(begin, end):
                    dispatch_copy(j, i, 1).start()

        def start_pass(j, begin=0, end=fine):
            for i in range(begin, end):
                u = j * fine + i
                for t in range(1, chips):
                    block = full.at[unit_slice(j, i), :, :, columns(across(t, -1))]
                    remote(
                        block, block, ys.at[u, t], yr.at[u, t], at(tp=across(t, -1))
                    ).wait_recv()
                    pass_on(j, i, t).start()

        def end_pass(j, begin=0, end=fine):
            for i in range(begin, end):
                u = j * fine + i
                block = full.at[unit_slice(j, i), :, :, columns(partner)]
                remote(block, block, ps.at[u], pr.at[u], at(tp=partner)).wait_recv()
                for t in range(1, chips):
                    block = full.at[
                        unit_slice(j, i), :, :, columns(turned(t, -1) * 2 + (1 - core))
                    ]
                    remote(block, block, fs.at[u, t], fr.at[u, t], at(tp=partner)).wait_recv()

        def chunk_rows(j):
            return pl.ds(pl.multiple_of(group_of(j, -1) * chunk, 16), chunk)

        def near_copy(j, t, p=0, count=pieces):
            base = group_of(j, -1) * chunk
            rows = pl.ds(pl.multiple_of(base + p * piece_rows, 16), count * piece_rows)
            return remote(
                part.at[rows, columns(turned(t, 1) * 2 + (1 - core))],
                near.at[j, t, piece(p, count)], ns.at[j, t, p], nr.at[j, t, p], at(tp=partner),
            )

        def piece(p, count=1):
            return pl.ds(pl.multiple_of(p * piece_rows, 16), count * piece_rows)

        def far_copy(j, t, i):
            return remote(
                total.at[j, t, piece(i)], far.at[j, t, piece(i)],
                ts.at[j, t, i], tr.at[j, t, i], at(tp=across(t, 1)),
            )

        def compute(j, p=0, count=pieces):
            base = group_of(j, -1)
            size = count * piece_rows
            where = pl.ds(pl.multiple_of(base * chunk + p * piece_rows, 16), size)
            sources = pl.ds(base * span + p * piece_sources, count * piece_sources)

            @pl.loop(0, hidden // hidden_block)
            def _(b):
                cut = pl.ds(pl.multiple_of(b * hidden_block, hidden_block), hidden_block)
                rows = full[sources, 0].reshape(size, full_width)
                pre_gate = jnp.dot(rows, wg[:, cut], preferred_element_type=f32)
                pre_up = jnp.dot(rows, wu[:, cut], preferred_element_type=f32)
                grads = full[sources, 1].reshape(size, full_width)
                act_grad = lax.dot_general(
                    grads, wd[cut, :], (((1,), (1,)), ((), ())), preferred_element_type=f32
                )
                sigmoid = jax.nn.sigmoid(pre_gate)
                silu = pre_gate * sigmoid
                slope = sigmoid * (1.0 + pre_gate * (1.0 - sigmoid))
                act[where, cut] = (silu * pre_up).astype(bf16)
                hid[0, where, cut] = (act_grad * pre_up * slope).astype(bf16)
                hid[1, where, cut] = (act_grad * silu).astype(bf16)

            @pl.loop(0, chips)
            def _(turn):
                t = lax.rem(turn + 1, chips)
                for side in ((1 - core), core):
                    cut = columns(turned(t, 1) * 2 + side)
                    value = lax.dot_general(
                        hid[0, where, :], wg[cut, :], (((1,), (1,)), ((), ())),
                        preferred_element_type=f32,
                    ) + lax.dot_general(
                        hid[1, where, :], wu[cut, :], (((1,), (1,)), ((), ())),
                        preferred_element_type=f32,
                    )
                    part[where, cut] = value.astype(bf16)
                    if side is not core:
                        near_copy(j, t, p, count).start()

        def add_near(j, t, p):
            where = pl.ds(pl.multiple_of(group_of(j, -1) * chunk + p * piece_rows, 16), piece_rows)
            value = part[where, columns(turned(t, 1) * 2 + core)].astype(f32) + near[
                j, t, piece(p)
            ].astype(f32)
            total[j, t, piece(p)] = value.astype(bf16)
            far_copy(j, t, p).start()

        def reduce_near(j):
            for t in list(range(1, chips)) + [0]:
                near_copy(j, t).wait_recv()
                if t > 0:
                    for p in range(pieces):
                        add_near(j, t, p)

        def reduce_near_piece(j, p):
            for t in list(range(1, chips)) + [0]:
                near_copy(j, t, p, 1).wait_recv()
                if t > 0:
                    add_near(j, t, p)

        def return_copy(j, source):
            turn = lax.rem(inner - source + span, span)
            k = j * span + turn
            other = group_of(j, -1) * span + source
            return k, remote(ret.at[other], rets.at[me], bs.at[k], br.at[k], at(sp=other))

        def reduce_far_piece(j, p):
            base = group_of(j, -1)
            where = pl.ds(pl.multiple_of(base * chunk + p * piece_rows, 16), piece_rows)
            value = part[where, mine].astype(f32) + near[j, 0, piece(p)].astype(f32)
            for t in range(1, chips):
                far_copy(j, t, p).wait_recv()
                value = value + far[j, t, piece(p)].astype(f32)
            ret[pl.ds(base * span + p * piece_sources, piece_sources)] = value.astype(
                bf16
            ).reshape(piece_sources, cap, width)
            for s in range(piece_sources):
                k, copy = return_copy(j, p * piece_sources + s)

                @pl.when(k > 0)
                def _():
                    copy.start()

        def reduce_far(j):
            for p in range(pieces):
                reduce_far_piece(j, p)

        if fine > 1:
            for copy in hand_over(0, 0):
                copy.start()

        @pl.loop(1, n)
        def _(k):
            j, i = k // span, k % span
            to = peer(j, i, 1)
            rows, grads = packed(to)
            send[to, 0] = rows
            send[to, 1] = grads

            @pl.when(j < 2)
            def _():
                dispatch_copy(j, i, 1).start()

        start_forward(0, 1 if fine > 1 else 0)
        release(2, 0, span)

        diagonal = lax.broadcasted_iota(jnp.int32, (channels, channels), 0) == (
            lax.broadcasted_iota(jnp.int32, (channels, channels), 1)
        )
        for d in range(2):
            column = jnp.sum(
                jnp.where(diagonal, lam_ref[d : d + 1, :], 0.0), axis=1, keepdims=True
            )
            speed[d] = decay_scale * softplus(-jnp.broadcast_to(column, (channels, 128)))
        token = lax.broadcasted_iota(jnp.int32, (block_width, length), 1)

        def shifted(value, by, d):
            return pltpu.roll(value, length - by if d == 0 else by, 1)

        def inside(by, d):
            return token < length - by if d == 0 else token >= by

        @pl.loop(0, blocks)
        def _(b):
            rows = pl.ds(pl.multiple_of(b * block_width, block_width), block_width)
            conv = conv_ref[rows, :]
            wide = conv.astype(f32)
            lru_out = jnp.zeros((block_width, length), f32)
            for d, state_ref in enumerate((before_ref, after_ref)):
                recur = jax.nn.sigmoid(
                    lax.dot_general(
                        wr_ref[d, b], conv, (((0,), (0,)), ((), ())), preferred_element_type=f32
                    )
                )
                inward = jax.nn.sigmoid(
                    lax.dot_general(
                        wi_ref[d, b], conv, (((0,), (0,)), ((), ())), preferred_element_type=f32
                    )
                )
                rate = speed[d, rows, 0:1]
                log_decay = jump_ref[rows, :] - rate * recur
                retain = jnp.exp(log_decay)
                root = jnp.sqrt(one_minus_exp(2.0 * log_decay, retain * retain))
                state = state_ref[rows, :]
                lru_out = lru_out + retain * state + root * inward * wide
                log_slope = state * retain - inward * wide * retain * retain / root
                slopes[d, 0, rows, :] = -rate * log_slope * recur * (1.0 - recur)
                slopes[d, 1, rows, :] = root * wide * inward * (1.0 - inward)
                slopes[d, 2, rows, :] = root * inward
                decay[d, rows, :] = retain
                product = retain
                for level, by in enumerate(levels):
                    keep = inside(by, d)
                    steps[d, level, rows, :] = jnp.where(keep, product, 0.0)
                    product = product * jnp.where(keep, shifted(product, by, d), 1.0)
                tails[d, rows, :] = jnp.where(inside(1, d), shifted(product, 1, d), 1.0)
                slopes[d, 3, rows, 0:128] = jnp.broadcast_to(
                    product[:, 0:1] if d == 0 else product[:, length - 1 : length],
                    (block_width, 128),
                )
            value = branch_ref[rows, :].astype(f32)
            scale = 0.7978845608028654
            tanh = jnp.tanh(scale * (value + 0.044715 * value * value * value))
            half = 0.5 * (1.0 + tanh)
            gelu = value * half
            slope = half + 0.5 * value * (1.0 - tanh * tanh) * scale * (
                1.0 + 3.0 * 0.044715 * value * value
            )
            mix_ref[rows, :] = (lru_out * gelu).astype(bf16)
            gelu_val[rows, :] = gelu
            gelu_slope[rows, :] = lru_out * slope

        for load in loads:
            load.wait()

        @pl.loop(0, groups - 1)
        def _(j):
            @pl.when(j < groups - 2)
            def _():
                start_forward(j + 1)
                release(j + 3, 0, half)

            @pl.when((j > 0) & (j < groups - 2))
            def _():
                release(j + 2, half, span)

            start_pass(j)
            end_pass(j)
            compute(j)

            @pl.when(j == groups - 2)
            def _():
                start_forward(groups - 1, 1)

            @pl.when(j > 0)
            def _():
                reduce_near(j)

            @pl.when(j == groups - 3)
            def _():
                start_forward(groups - 1, 0, 1)

            @pl.when(j > 1)
            def _():
                reduce_far(j - 1)

        final = groups - 1
        if split_last:
            early, late = lax.rem(inner + span, span), lax.rem(inner + span - 1, span)
            start_pass(final, 0, 1)
            end_pass(final, 0, 1)
            compute(final, early, 1)
            start_pass(final, 1)
            reduce_near_piece(final, early)
            end_pass(final, 1)
            compute(final, late, 1)
            reduce_near_piece(final, late)
            reduce_near(0)
            reduce_far(final - 1)
            reduce_far_piece(final, early)
        else:
            late = pieces - 1
            start_pass(final)
            end_pass(final)
            compute(final)
            reduce_near(final)
            reduce_near(0)
            reduce_far(final - 1)
            for p in range(pieces - 1):
                reduce_far_piece(final, p)
        first_contract = (((0,), (0,)), ((), ()))

        grad_blocks = full_width // grad_block
        middle = grad_blocks * 3 // 4
        for begin, end in ((0, middle), (middle, grad_blocks)):
            @pl.loop(begin, end)
            def _(b):
                cut = pl.ds(pl.multiple_of(b * grad_block, grad_block), grad_block)
                rows = full[:, 0, :, cut].reshape(total_rows, grad_block)
                gate_out[cut, :] = lax.dot_general(
                    rows, hid[0], first_contract, preferred_element_type=f32
                ).astype(bf16)
                up_out[cut, :] = lax.dot_general(
                    rows, hid[1], first_contract, preferred_element_type=f32
                ).astype(bf16)

            with jax.named_scope("S3"):
                if begin == 0:
                    reduce_far_piece(final, late)
                else:
                    reduce_far(0)
                    rets[me] = ret[me]

        @pl.loop(0, full_width // grad_block)
        def _(b):
            cut = pl.ds(pl.multiple_of(b * grad_block, grad_block), grad_block)
            grads = full[:, 1, :, cut].reshape(total_rows, grad_block)
            down_out[:, cut] = lax.dot_general(
                act[...], grads, first_contract, preferred_element_type=f32
            ).astype(bf16)

        @pl.loop(1, n)
        def _(k):
            j, i = k // span, k % span
            other = peer(j, i, 1)
            remote(ret.at[other], rets.at[other], bs.at[k], br.at[k], at(sp=other)).wait_recv()

        back = lax.dot_general(
            pick[...], rets[...].reshape(total_rows, width), first_contract,
            preferred_element_type=f32,
        )
        residual = (cot_ref[...].astype(f32) + back).astype(bf16)
        res_ref[...] = residual
        fullres_ref[:, mine] = residual

        def half_columns(member, h):
            return pl.ds(pl.multiple_of(member * width + h * half_width, half_width), half_width)

        def half_of(h):
            return (1 - inner if h == 0 else inner) if halves == 2 else 0

        def gather_copy(t, h):
            block = fullres_ref.at[:, half_columns(place, half_of(h))]
            to = partner if t == 0 else across(t, 1)
            return remote(block, block, gs.at[t, h], gr.at[t, h], at(tp=to))

        def gather_wait(t, h):
            origin = partner if t == 0 else across(t, -1)
            block = fullres_ref.at[:, half_columns(origin, half_of(h))]
            return remote(block, block, gs.at[t, h], gr.at[t, h], at(tp=origin))

        def gather_pass(t, h):
            block = fullres_ref.at[:, half_columns(across(t, -1), half_of(h))]
            return remote(block, block, hs.at[t, h], hr.at[t, h], at(tp=partner))

        def pass_wait(t, h):
            block = fullres_ref.at[
                :, half_columns(turned(t, -1) * 2 + (1 - core), half_of(h))
            ]
            return remote(block, block, hs.at[t, h], hr.at[t, h], at(tp=partner))

        for h in range(halves):
            for t in range(1, chips):
                gather_copy(t, h).start()
        for h in range(halves):
            gather_copy(0, h).start()

        def strip_of(g, i):
            other = g * span + i
            if upright:
                return proj_part.at[:, pl.ds(pl.multiple_of(other * strip, strip), strip)]
            return proj_part.at[pl.ds(pl.multiple_of(other * strip, strip), strip), :]

        def read_strip(other):
            where = pl.ds(pl.multiple_of(other * strip, strip), strip)
            return (proj_part[:, where] if upright else proj_part[where, :]).astype(f32)

        def inner_peer(i, sign):
            return lax.rem(inner + sign * i + span, span)

        def outer_peer(g, sign):
            return lax.rem(group + sign * g + groups, groups)

        def inner_copy(g, i):
            other = outer_peer(g, 1)
            return remote(
                strip_of(other, inner_peer(i, 1)), proj_near.at[g, i], xs.at[g, i], xr.at[g, i],
                at(sp=group * span + inner_peer(i, 1)),
            )

        def outer_copy(g):
            return remote(
                proj_sum.at[g], proj_far.at[g], zs.at[g], zr.at[g],
                at(sp=outer_peer(g, 1) * span + inner),
            )

        turns = list(range(1, groups))
        turns = sorted(turns, key=lambda g: abs(g - groups // 2)) + [0]
        turn_width = span * strip

        def project(g):
            where = pl.ds(pl.multiple_of(outer_peer(g, 1) * turn_width, turn_width), turn_width)
            if upright:
                proj_part[:, where] = jnp.dot(
                    mix_ref[...], fullres_ref[:, where], preferred_element_type=f32
                ).astype(bf16)
            else:
                proj_part[where, :] = lax.dot_general(
                    fullres_ref[:, where], mix_ref[...], (((0,), (1,)), ((), ())),
                    preferred_element_type=f32,
                ).astype(bf16)
            for i in range(1, span):
                inner_copy(g, i).start()

        def project_half(member, h):
            where = half_columns(member, half_of(h))
            proj_part[:, where] = jnp.dot(
                mix_ref[...], fullres_ref[:, where], preferred_element_type=f32
            ).astype(bf16)
            if h == 0:
                inner_copy(lax.rem(member - group + groups, groups), 1).start()

        def finish_inner(g):
            total_strip = read_strip(outer_peer(g, 1) * span + inner)
            for i in range(1, span):
                inner_copy(g, i).wait_recv()
                total_strip = total_strip + proj_near[g, i].astype(f32)
            proj_sum[g] = total_strip.astype(bf16)

            @pl.when(g > 0)
            def _():
                outer_copy(g).start()

        other_side = turned(1, -1) * 2
        if halves == 2:
            project_half(place, 0)
            gather_wait(1, 0).wait_recv()
            gather_pass(1, 0).start()
            project_half(other_side + core, 0)
            pass_wait(1, 0).wait_recv()
            project_half(other_side + (1 - core), 0)
            gather_wait(0, 0).wait_recv()
            project_half(partner, 0)
            project_half(place, 1)
            finish_inner(lax.rem(place - group + groups, groups))
            gather_wait(1, 1).wait_recv()
            gather_pass(1, 1).start()
            gather_wait(0, 1).wait_recv()
            project_half(partner, 1)
            project_half(other_side + core, 1)
            pass_wait(1, 1).wait_recv()
            project_half(other_side + (1 - core), 1)
        else:
            for t in range(1, chips):
                gather_wait(t, 0).wait_recv()
                gather_pass(t, 0).start()
            gather_wait(0, 0).wait_recv()
            for t in range(1, chips):
                pass_wait(t, 0).wait_recv()
            for g in turns[:2]:
                project(g)
        mix_grad[...] = lax.dot_general(
            outp_ref[...], fullres_ref[...], (((1,), (1,)), ((), ())), preferred_element_type=f32
        )
        lane = lax.broadcasted_iota(jnp.int32, (block_width, 128), 1)

        @pl.loop(0, blocks)
        def _(b):
            rows = pl.ds(pl.multiple_of(b * block_width, block_width), block_width)
            upper = mix_grad[rows, :]
            branch_out[rows, :] = upper * gelu_slope[rows, :]
            grad = upper * gelu_val[rows, :]
            last = []
            for d in range(2):
                carried = decay[d, rows, :] * grad
                for level, by in enumerate(levels):
                    carried = carried + steps[d, level, rows, :] * shifted(carried, by, d)
                local[d, rows, :] = grad + jnp.where(inside(1, d), shifted(carried, 1, d), 0.0)
                last.append(carried[:, 0:1] if d == 0 else carried[:, length - 1 : length])
            packed_ends = jnp.where(lane == 0, last[0], jnp.where(lane == 1, last[1], 0.0))
            packed_ends = jnp.where(lane == 2, slopes[0, 3, rows, 0:128], packed_ends)
            ends[rows, :] = jnp.where(lane == 3, slopes[1, 3, rows, 0:128], packed_ends)

        if channels < channels_pad:
            ends[channels:, :] = jnp.zeros((channels_pad - channels, 128), f32)
        ends_row[...] = ends[...].T[0:8, :]

        def ends_copy(k):
            return remote(
                ends_row, ends_all.at[me], es.at[k], er.at[k], at(sp=lax.rem(me + k, n))
            )

        @pl.loop(1, n)
        def _(k):
            ends_copy(k).start()

        ends_all[me] = ends_row[...]

        if halves == 2:
            finish_inner(lax.rem(other_side + core - group + groups, groups))
            finish_inner(lax.rem(other_side + (1 - core) - group + groups, groups))
            finish_inner(lax.rem(partner - group + groups, groups))
        else:
            for g in turns[2:]:
                project(g)
            for g in turns[:-2]:
                finish_inner(g)
        @pl.loop(1, n)
        def _(k):
            origin = lax.rem(me - k + n, n)
            remote(
                ends_row, ends_all.at[origin], es.at[k], er.at[k], at(sp=origin)
            ).wait_recv()

        incoming = [jnp.zeros((1, channels_pad), f32)] * 2
        for turn in range(n - 1):
            late = n - 1 - turn
            incoming[0] = jnp.where(
                late > me, ends_all[late, 2:3, :] * incoming[0] + ends_all[late, 0:1, :], incoming[0]
            )
            incoming[1] = jnp.where(
                turn < me, ends_all[turn, 3:4, :] * incoming[1] + ends_all[turn, 1:2, :], incoming[1]
            )
        line = lax.broadcasted_iota(jnp.int32, (128, channels_pad), 0)
        carry[...] = jnp.where(line == 0, incoming[0], jnp.where(line == 1, incoming[1], 0.0)).T

        @pl.loop(0, blocks)
        def _(b):
            rows = pl.ds(pl.multiple_of(b * block_width, block_width), block_width)
            value = jnp.zeros((block_width, length), f32)
            for d in range(2):
                delta = local[d, rows, :] + tails[d, rows, :] * carry[rows, d : d + 1]
                value = value + delta * slopes[d, 2, rows, :]
                value = value + jnp.dot(
                    wr_ref[d, b], (delta * slopes[d, 0, rows, :]).astype(bf16),
                    preferred_element_type=f32,
                )
                value = value + jnp.dot(
                    wi_ref[d, b], (delta * slopes[d, 1, rows, :]).astype(bf16),
                    preferred_element_type=f32,
                )
            conv_out[rows, :] = value

        if halves == 1:
            for g in turns[-2:]:
                finish_inner(g)
        summed = proj_sum[0].astype(f32)
        for g in turns[:-1]:
            outer_copy(g).wait_recv()
            summed = summed + proj_far[g].astype(f32)
        proj_ref[...] = summed if upright else summed.T

        for g in turns:
            for i in range(1, span):
                inner_copy(g, i).wait_send()
            if g > 0:
                outer_copy(g).wait_send()

        @pl.loop(1, n)
        def _(k):
            ends_copy(k).wait_send()

        @pl.loop(1, n)
        def _(k):
            j, i = k // span, k % span
            dispatch_copy(j, i, 1).wait_send()
            source = peer(j, i, -1)
            remote(ret.at[source], rets.at[me], bs.at[k], br.at[k], at(sp=source)).wait_send()

        @pl.loop(0, groups)
        def _(j):
            for i in range(fine):
                for copy in hand_over(j, i):
                    copy.wait_send()
                for t in range(1, chips):
                    pass_on(j, i, t).wait_send()
            for t in range(chips):
                if split_last:
                    for p in range(pieces):
                        @pl.when(j == groups - 1)
                        def _():
                            near_copy(j, t, p, 1).wait_send()

                    @pl.when(j < groups - 1)
                    def _():
                        near_copy(j, t).wait_send()
                else:
                    near_copy(j, t).wait_send()
            for t in range(1, chips):
                for p in range(pieces):
                    far_copy(j, t, p).wait_send()

        for h in range(halves):
            for t in range(chips):
                gather_copy(t, h).wait_send()
            for t in range(1, chips):
                gather_pass(t, h).wait_send()


    dma = pltpu.SemaphoreType.DMA
    wide = max(chips, 2)
    sem = lambda *shape: [dma(shape)] * 2
    any_spec = pl.BlockSpec(memory_space=pl.ANY)
    shape = jax.ShapeDtypeStruct
    strip_shape = (channels, strip) if upright else (strip, channels)
    part_shape = (channels, full_width) if upright else (full_width, channels)
    return pl.pallas_call(
        kernel, name="layer_backward",
        out_shape=(
            pltpu.VMEM((tokens, width), bf16), pltpu.VMEM((channels, strip), f32),
            pltpu.VMEM((channels, length), f32), pltpu.VMEM((channels, length), f32),
            pltpu.VMEM(w_gate.shape, bf16), pltpu.VMEM(w_up.shape, bf16), pltpu.VMEM(w_down.shape, bf16),
        ),
        in_specs=[VMEM_SPEC] * 13 + [any_spec] * 3,
        out_specs=(VMEM_SPEC,) * 7,
        scratch_shapes=[
            pltpu.VMEM(w_gate.shape, bf16), pltpu.VMEM(w_up.shape, bf16), pltpu.VMEM(w_down.shape, bf16),
            pltpu.VMEM((128, tokens), f32), pltpu.VMEM((128, tokens), f32),
            pltpu.VMEM((total_rows, tokens), bf16),
            pltpu.VMEM((n, 2, cap, width), bf16),
            pltpu.VMEM((n, 2, cap, full_width), bf16),
            pltpu.VMEM((2, total_rows, hidden), bf16),
            pltpu.VMEM((total_rows, hidden), bf16),
            pltpu.VMEM((total_rows, full_width), bf16),
            pltpu.VMEM((groups, chips, chunk, width), bf16),
            pltpu.VMEM((groups, chips, chunk, width), bf16),
            pltpu.VMEM((groups, chips, chunk, width), bf16),
            pltpu.VMEM((n, cap, width), bf16), pltpu.VMEM((n, cap, width), bf16),
            pltpu.VMEM((tokens, full_width), bf16),
            pltpu.VMEM((2, 4, channels, length), f32),
            pltpu.VMEM((2, len(levels), channels, length), f32),
            pltpu.VMEM((2, channels, length), f32), pltpu.VMEM((2, channels, length), f32),
            pltpu.VMEM((2, channels, 128), f32),
            pltpu.VMEM((channels, length), bf16),
            pltpu.VMEM((channels, length), f32), pltpu.VMEM((channels, length), f32),
            pltpu.VMEM((channels, length), f32), pltpu.VMEM((2, channels, length), f32),
            pltpu.VMEM((channels_pad, 128), f32), pltpu.VMEM((8, channels_pad), f32),
            pltpu.VMEM((n, 8, channels_pad), f32), pltpu.VMEM((channels_pad, 128), f32),
            pltpu.VMEM(part_shape, bf16),
            pltpu.VMEM((groups, span) + strip_shape, bf16),
            pltpu.VMEM((groups,) + strip_shape, bf16), pltpu.VMEM((groups,) + strip_shape, bf16),
        ]
        + sem(n) + sem(groups, span) + sem(groups)
        + [dma((3,))]
        + sem(n) + sem(units, wide) + sem(units) + sem(units, wide)
        + sem(groups, wide, pieces) + sem(groups, wide, pieces) + sem(n) + sem(wide, halves) + sem(wide, halves),
        compiler_params=pltpu.CompilerParams(
            collective_id=1, has_side_effects=True, vmem_limit_bytes=54 * 1024 * 1024
        ),
    )(
        cotangent, moe_input, routes.T, gates.T, conv_in, branch, state_before, state_after, jump,
        recur_weight, input_weight, lam, out_proj, w_gate, w_up, w_down,
    )


def write_out(values):
    count = len(values)

    def kernel(*refs):
        sems = refs[2 * count]
        copies = [
            pltpu.make_async_copy(refs[i], refs[count + i], sems.at[i]) for i in range(count)
        ]
        for copy in copies:
            copy.start()
        for copy in copies:
            copy.wait()

    return pl.pallas_call(
        kernel, name="write_out",
        out_shape=tuple(jax.ShapeDtypeStruct(v.shape, v.dtype) for v in values),
        in_specs=[pl.BlockSpec(memory_space=pl.ANY)] * count,
        out_specs=(pl.BlockSpec(memory_space=pl.ANY),) * count,
        scratch_shapes=[pltpu.SemaphoreType.DMA((count,))],
        compiler_params=pltpu.CompilerParams(vmem_limit_bytes=4 * 1024 * 1024),
    )(*values)


def on_device(
    cotangent, moe_input, routes, gates, w_gate, w_up, w_down, out_proj, conv_in, branch,
    state_before, state_after, jump, recur_weight, input_weight, lam,
):
    residual_grad, out_proj_grad, conv_grad, branch_grad, gate_grad, up_grad, down_grad = (
        write_out(layer_backward(
            cotangent, moe_input, routes, gates, w_gate[0], w_up[0], w_down[0], out_proj, conv_in,
            branch, state_before, state_after, jump, recur_weight, input_weight, lam,
        ))
    )
    return (
        gate_grad[None], up_grad[None], down_grad[None],
        residual_grad, out_proj_grad, conv_grad, branch_grad,
    )


def solution(mesh):
    placed = (
        P("sp", "tp"),
        P("sp", "tp"),
        P("sp", None),
        P("sp", None),
        P("sp", None, "tp"),
        P("sp", None, "tp"),
        P("sp", "tp", None),
        P("tp", None),
        P("tp", "sp"),
        P("tp", "sp"),
        P("tp", "sp"),
        P("tp", "sp"),
        P("tp", "sp"),
        P(None, "tp", None, None),
        P(None, "tp", None, None),
        P(None, "tp"),
    )
    return jax.shard_map(
        on_device,
        mesh=mesh,
        in_specs=placed,
        out_specs=(
            P("sp", None, "tp"),
            P("sp", None, "tp"),
            P("sp", "tp", None),
            P("sp", "tp"),
            P("tp", "sp"),
            P("tp", "sp"),
            P("tp", "sp"),
        ),
        check_vma=False,
    )
```

```python
import jax
import jax.numpy as jnp
from jax import lax
from jax.experimental import pallas as pl
from jax.experimental.pallas import tpu as pltpu
from jax.sharding import PartitionSpec as P

decay_scale = 8.0


MESH = pl.DeviceIdType.MESH
VMEM_SPEC = pl.BlockSpec(memory_space=pltpu.VMEM)


def at(sp=None, tp=None):
    sp = lax.axis_index("sp") if sp is None else sp
    tp = lax.axis_index("tp") if tp is None else tp
    return (sp, tp)


def greet(devices):
    barrier = pltpu.get_barrier_semaphore()
    for device in devices:
        pl.semaphore_signal(barrier, inc=1, device_id=device, device_id_type=MESH)


def await_greetings(count):
    pl.semaphore_wait(pltpu.get_barrier_semaphore(), count)


def remote(source, target, send, recv, device):
    return pltpu.make_async_remote_copy(
        src_ref=source, dst_ref=target, send_sem=send, recv_sem=recv,
        device_id=device, device_id_type=MESH,
    )


def softplus(value):
    small = jnp.exp(-jnp.abs(value))
    series = small * (1.0 - small * (0.5 - small * (1.0 / 3.0 - small * 0.25)))
    return jnp.maximum(value, 0.0) + jnp.where(small < 0.01, series, jnp.log(1.0 + small))


def one_minus_exp(value, exponential):
    series = -value * (
        1.0 + value * (0.5 + value * (1.0 / 6.0 + value * (1.0 / 24.0 + value * (
            1.0 / 120.0 + value * (1.0 / 720.0)
        ))))
    )
    return jnp.where(value > -0.25, series, 1.0 - exponential)


def layer_backward(
    cotangent, moe_input, routes, gates, w_gate, w_up, w_down, out_proj, conv_in, branch,
    state_before, state_after, jump, recur_weight, input_weight, lam,
):
    n, tp = lax.axis_size("sp"), lax.axis_size("tp")
    chips = tp // 2
    tokens, width = cotangent.shape
    full_width, hidden = w_gate.shape
    cap = -(-(3 * tokens // n) // 16) * 16
    span = min(n, 2 if n <= 8 else 4)
    groups = n // span
    fine = span if n <= 8 else 1
    per_unit = span // fine
    units = groups * fine
    chunk = span * cap
    total_rows = n * cap
    pieces = 2 if span % 2 == 0 else 1
    piece_rows, piece_sources = chunk // pieces, span // pieces
    split_last = fine == 2 and pieces == 2
    hidden_block = min(hidden, 256)
    column_block = min(full_width, 512)
    grad_block = min(full_width, 256)
    f32, bf16 = jnp.float32, jnp.bfloat16
    channels, length = conv_in.shape
    blocks, block_width = recur_weight.shape[1:3]
    channels_pad = max(channels, 128)
    strip = full_width // n
    upright = strip % 128 == 0
    halves = 2 if span == 2 and chips == 2 and groups == tp and upright else 1
    half_width = width // halves
    quarters = 2 if halves == 2 and strip % 256 == 0 else 1
    quarter_width, slice_width = half_width // quarters, strip // quarters
    scan_rows = min(channels, 128)
    levels = [1 << i for i in range((length - 1).bit_length())]

    def kernel(
        cot_ref, in_ref, routes_ref, gates_ref, conv_ref, branch_ref, before_ref, after_ref,
        jump_ref, wr_ref, wi_ref, lam_ref, outp_ref, wg_hbm, wu_hbm, wd_hbm,
        res_ref, proj_ref, conv_out, branch_out, gate_out, up_out, down_out,
        wg, wu, wd, wg_t, wu_t, wd_t, key_t, gate_t, pick, send, full, hid, act, part, near, total, far, ret, rets,
        fullres_ref,
        slopes, steps, decay, tails, speed, mix_ref, gelu_val, gelu_slope, mix_grad, local,
        ends, ends_row, ends_all, carry, proj_part, proj_near, proj_sum, proj_far,
        es, er, xs, xr, zs, zr,
        ws, ss, sr, ys, yr, ps, pr, fs, fr, ns, nr, ts, tr, bs, br, gs, gr, hs, hr,
    ):
        me, place = lax.axis_index("sp"), lax.axis_index("tp")
        chip, core = place // 2, place % 2
        partner = chip * 2 + (1 - core)
        group, inner = me // span, me % span

        def columns(member):
            return pl.ds(pl.multiple_of(member * width, width), width)

        mine = columns(place)

        def turned(t, sign):
            return lax.rem(chip + sign * t + chips, chips)

        def across(t, sign):
            return turned(t, sign) * 2 + core

        def order(j):
            return jnp.where(j < 2, j, groups + 1 - j)

        def group_of(j, sign):
            return lax.rem(group + sign * order(j) + groups, groups)

        def peer(j, i, sign):
            return group_of(j, sign) * span + lax.rem(inner + sign * i + span, span)

        weights = ((wg_hbm, wg), (wu_hbm, wu), (wd_hbm, wd))
        loads = [pltpu.make_async_copy(a, b, ws.at[i]) for i, (a, b) in enumerate(weights)]
        for load in loads:
            load.start()

        greet(
            [at(sp=lax.rem(me + k, n)) for k in range(1, n)]
            + [at(tp=partner)]
            + [at(tp=across(t, 1)) for t in range(1, chips)]
        )

        expert_id = lax.broadcasted_iota(jnp.int32, (128, tokens), 0)
        first = expert_id == routes_ref[0:1, :]
        second = expert_id == routes_ref[1:2, :]
        member = jnp.where(first | second, 1.0, 0.0).astype(f32)
        gate_t[...] = jnp.where(first, gates_ref[0:1, :], 0.0) + jnp.where(
            second, gates_ref[1:2, :], 0.0
        )
        earlier = lax.broadcasted_iota(jnp.int32, (tokens, tokens), 0) < lax.broadcasted_iota(
            jnp.int32, (tokens, tokens), 1
        )
        earlier = jnp.where(earlier, 1.0, 0.0).astype(bf16)
        position = jnp.dot(member.astype(bf16), earlier, preferred_element_type=f32)
        key_t[...] = jnp.where(member > 0.5, position, -1.0)
        row_id = lax.broadcasted_iota(jnp.int32, (cap, tokens), 0).astype(f32)

        def packed(to):
            chosen = row_id == key_t[pl.ds(to, 1), :]
            one_hot = jnp.where(chosen, 1.0, 0.0).astype(bf16)
            scale = jnp.sum(jnp.where(chosen, gate_t[pl.ds(to, 1), :], 0.0), axis=1, keepdims=True)
            pick[pl.ds(pl.multiple_of(to * cap, 16), cap), :] = one_hot
            rows = jnp.dot(one_hot, in_ref[...], preferred_element_type=f32).astype(bf16)
            grads = jnp.dot(one_hot, cot_ref[...], preferred_element_type=f32) * scale
            return rows, grads.astype(bf16)

        rows, grads = packed(me)
        full[me, 0, :, mine] = rows
        full[me, 1, :, mine] = grads

        def unit_slice(j, i):
            base = group_of(j, -1) * span
            if fine > 1:
                return pl.ds(base + lax.rem(inner - i + span, span), 1)
            return pl.ds(base, span)

        def dispatch_copy(j, i, sign):
            other = peer(j, i, sign)
            k = j * span + i
            return remote(
                send.at[other], full.at[me if sign > 0 else other, :, :, mine],
                ss.at[k], sr.at[k], at(sp=other),
            )

        def hand_over(j, i):
            block = full.at[unit_slice(j, i), :, :, mine]
            u = j * fine + i
            out = [
                remote(block, block, ys.at[u, t], yr.at[u, t], at(tp=across(t, 1)))
                for t in range(1, chips)
            ]
            out.append(remote(block, block, ps.at[u], pr.at[u], at(tp=partner)))
            return out

        def pass_on(j, i, t):
            block = full.at[unit_slice(j, i), :, :, columns(across(t, -1))]
            u = j * fine + i
            return remote(block, block, fs.at[u, t], fr.at[u, t], at(tp=partner))

        def start_forward(j, begin=0, end=fine):
            for i in range(begin, min(end, fine)):
                for s in range(per_unit):
                    number = i * per_unit + s

                    @pl.when(j * span + number > 0)
                    def _():
                        dispatch_copy(j, number, -1).wait_recv()

                for copy in hand_over(j, i):
                    copy.start()

        half = span // 2

        def release(j, begin, end):
            @pl.when(j < groups)
            def _():
                for i in range(begin, end):
                    dispatch_copy(j, i, 1).start()

        def start_pass(j, begin=0, end=fine):
            for i in range(begin, end):
                u = j * fine + i
                for t in range(1, chips):
                    block = full.at[unit_slice(j, i), :, :, columns(across(t, -1))]
                    remote(
                        block, block, ys.at[u, t], yr.at[u, t], at(tp=across(t, -1))
                    ).wait_recv()
                    pass_on(j, i, t).start()

        def end_pass(j, begin=0, end=fine):
            for i in range(begin, end):
                u = j * fine + i
                block = full.at[unit_slice(j, i), :, :, columns(partner)]
                remote(block, block, ps.at[u], pr.at[u], at(tp=partner)).wait_recv()
                for t in range(1, chips):
                    block = full.at[
                        unit_slice(j, i), :, :, columns(turned(t, -1) * 2 + (1 - core))
                    ]
                    remote(block, block, fs.at[u, t], fr.at[u, t], at(tp=partner)).wait_recv()

        def chunk_rows(j):
            return pl.ds(pl.multiple_of(group_of(j, -1) * chunk, 16), chunk)

        def near_copy(j, t, p=0, count=pieces):
            base = group_of(j, -1) * chunk
            rows = pl.ds(pl.multiple_of(base + p * piece_rows, 16), count * piece_rows)
            return remote(
                part.at[rows, columns(turned(t, 1) * 2 + (1 - core))],
                near.at[j, t, piece(p, count)], ns.at[j, t, p], nr.at[j, t, p], at(tp=partner),
            )

        def piece(p, count=1):
            return pl.ds(pl.multiple_of(p * piece_rows, 16), count * piece_rows)

        def far_copy(j, t, i):
            return remote(
                total.at[j, t, piece(i)], far.at[j, t, piece(i)],
                ts.at[j, t, i], tr.at[j, t, i], at(tp=across(t, 1)),
            )

        def compute(j, p=0, count=pieces):
            base = group_of(j, -1)
            size = count * piece_rows
            where = pl.ds(pl.multiple_of(base * chunk + p * piece_rows, 16), size)
            sources = pl.ds(base * span + p * piece_sources, count * piece_sources)

            @pl.loop(0, hidden // hidden_block)
            def _(b):
                cut = pl.ds(pl.multiple_of(b * hidden_block, hidden_block), hidden_block)
                rows = full[sources, 0].reshape(size, full_width)
                pre_gate = jnp.dot(rows, wg[:, cut], preferred_element_type=f32)
                pre_up = jnp.dot(rows, wu[:, cut], preferred_element_type=f32)
                grads = full[sources, 1].reshape(size, full_width)
                act_grad = jnp.dot(grads, wd_t[:, cut], preferred_element_type=f32)
                sigmoid = jax.nn.sigmoid(pre_gate)
                silu = pre_gate * sigmoid
                slope = sigmoid * (1.0 + pre_gate * (1.0 - sigmoid))
                act[where, cut] = (silu * pre_up).astype(bf16)
                hid[0, where, cut] = (act_grad * pre_up * slope).astype(bf16)
                hid[1, where, cut] = (act_grad * silu).astype(bf16)

            @pl.loop(0, chips)
            def _(turn):
                t = lax.rem(turn + 1, chips)
                for side in ((1 - core), core):
                    cut = columns(turned(t, 1) * 2 + side)
                    value = jnp.dot(
                        hid[0, where, :], wg_t[:, cut], preferred_element_type=f32
                    ) + jnp.dot(hid[1, where, :], wu_t[:, cut], preferred_element_type=f32)
                    part[where, cut] = value.astype(bf16)
                    if side is not core:
                        near_copy(j, t, p, count).start()

        def add_near(j, t, p):
            where = pl.ds(pl.multiple_of(group_of(j, -1) * chunk + p * piece_rows, 16), piece_rows)
            value = part[where, columns(turned(t, 1) * 2 + core)].astype(f32) + near[
                j, t, piece(p)
            ].astype(f32)
            total[j, t, piece(p)] = value.astype(bf16)
            far_copy(j, t, p).start()

        def reduce_near(j):
            for t in list(range(1, chips)) + [0]:
                near_copy(j, t).wait_recv()
                if t > 0:
                    for p in range(pieces):
                        add_near(j, t, p)

        def reduce_near_piece(j, p):
            for t in list(range(1, chips)) + [0]:
                near_copy(j, t, p, 1).wait_recv()
                if t > 0:
                    add_near(j, t, p)

        def return_copy(j, source):
            turn = lax.rem(inner - source + span, span)
            k = j * span + turn
            other = group_of(j, -1) * span + source
            return k, remote(ret.at[other], rets.at[me], bs.at[k], br.at[k], at(sp=other))

        def reduce_far_piece(j, p):
            base = group_of(j, -1)
            where = pl.ds(pl.multiple_of(base * chunk + p * piece_rows, 16), piece_rows)
            value = part[where, mine].astype(f32) + near[j, 0, piece(p)].astype(f32)
            for t in range(1, chips):
                far_copy(j, t, p).wait_recv()
                value = value + far[j, t, piece(p)].astype(f32)
            ret[pl.ds(base * span + p * piece_sources, piece_sources)] = value.astype(
                bf16
            ).reshape(piece_sources, cap, width)
            for s in range(piece_sources):
                k, copy = return_copy(j, p * piece_sources + s)

                @pl.when(k > 0)
                def _():
                    copy.start()

        def reduce_far(j):
            for p in range(pieces):
                reduce_far_piece(j, p)

        @pl.loop(1, n)
        def _(k):
            to = peer(k // span, k % span, 1)
            rows, grads = packed(to)
            send[to, 0] = rows
            send[to, 1] = grads

        await_greetings(n + chips - 1)
        if fine > 1:
            for copy in hand_over(0, 0):
                copy.start()

        @pl.loop(1, 2 * span)
        def _(k):
            dispatch_copy(k // span, k % span, 1).start()

        for load in loads:
            load.wait()

        @pl.loop(0, full_width // grad_block)
        def _(b):
            cut = pl.ds(pl.multiple_of(b * grad_block, grad_block), grad_block)
            wd_t[cut, :] = wd[:, cut].T
            wg_t[:, cut] = wg[cut, :].T
            wu_t[:, cut] = wu[cut, :].T

        start_forward(0, 1 if fine > 1 else 0)
        release(2, 0, span)

        diagonal = lax.broadcasted_iota(jnp.int32, (channels, channels), 0) == (
            lax.broadcasted_iota(jnp.int32, (channels, channels), 1)
        )
        for d in range(2):
            column = jnp.sum(
                jnp.where(diagonal, lam_ref[d : d + 1, :], 0.0), axis=1, keepdims=True
            )
            speed[d] = decay_scale * softplus(-jnp.broadcast_to(column, (channels, 128)))

        def shifted(value, by, d):
            return pltpu.roll(value, length - by if d == 0 else by, 1)

        def inside(by, d, rows=block_width):
            token = lax.broadcasted_iota(jnp.int32, (rows, length), 1)
            return token < length - by if d == 0 else token >= by

        @pl.loop(0, blocks)
        def _(b):
            rows = pl.ds(pl.multiple_of(b * block_width, block_width), block_width)
            conv = conv_ref[rows, :]
            wide = conv.astype(f32)
            lru_out = jnp.zeros((block_width, length), f32)
            for d, state_ref in enumerate((before_ref, after_ref)):
                recur = jax.nn.sigmoid(
                    lax.dot_general(
                        wr_ref[d, b], conv, (((0,), (0,)), ((), ())), preferred_element_type=f32
                    )
                )
                inward = jax.nn.sigmoid(
                    lax.dot_general(
                        wi_ref[d, b], conv, (((0,), (0,)), ((), ())), preferred_element_type=f32
                    )
                )
                rate = speed[d, rows, 0:1]
                log_decay = jump_ref[rows, :] - rate * recur
                retain = jnp.exp(log_decay)
                root = jnp.sqrt(one_minus_exp(2.0 * log_decay, retain * retain))
                state = state_ref[rows, :]
                lru_out = lru_out + retain * state + root * inward * wide
                log_slope = state * retain - inward * wide * retain * retain / root
                slopes[d, 0, rows, :] = -rate * log_slope * recur * (1.0 - recur)
                slopes[d, 1, rows, :] = root * wide * inward * (1.0 - inward)
                slopes[d, 2, rows, :] = root * inward
                decay[d, rows, :] = retain
                product = retain
                for level, by in enumerate(levels):
                    keep = inside(by, d)
                    steps[d, level, rows, :] = jnp.where(keep, product, 0.0)
                    product = product * jnp.where(keep, shifted(product, by, d), 1.0)
                tails[d, rows, :] = jnp.where(inside(1, d), shifted(product, 1, d), 1.0)
                slopes[d, 3, rows, 0:128] = jnp.broadcast_to(
                    product[:, 0:1] if d == 0 else product[:, length - 1 : length],
                    (block_width, 128),
                )
            value = branch_ref[rows, :].astype(f32)
            scale = 0.7978845608028654
            tanh = jnp.tanh(scale * (value + 0.044715 * value * value * value))
            half = 0.5 * (1.0 + tanh)
            gelu = value * half
            slope = half + 0.5 * value * (1.0 - tanh * tanh) * scale * (
                1.0 + 3.0 * 0.044715 * value * value
            )
            mix_ref[rows, :] = (lru_out * gelu).astype(bf16)
            gelu_val[rows, :] = gelu
            gelu_slope[rows, :] = lru_out * slope


        @pl.loop(0, groups - 1)
        def _(j):
            @pl.when(j < groups - 2)
            def _():
                start_forward(j + 1)
                release(j + 3, 0, half)

            @pl.when((j > 0) & (j < groups - 2))
            def _():
                release(j + 2, half, span)

            start_pass(j)
            end_pass(j)
            compute(j)

            @pl.when(j == groups - 2)
            def _():
                start_forward(groups - 1, 1)

            @pl.when(j > 0)
            def _():
                reduce_near(j)

            @pl.when(j == groups - 3)
            def _():
                start_forward(groups - 1, 0, 1)

            @pl.when(j > 1)
            def _():
                reduce_far(j - 1)

        final = groups - 1
        if split_last:
            early, late = lax.rem(inner + span, span), lax.rem(inner + span - 1, span)
            start_pass(final, 0, 1)
            end_pass(final, 0, 1)
            compute(final, early, 1)
            start_pass(final, 1)
            reduce_near_piece(final, early)
            end_pass(final, 1)
            compute(final, late, 1)
            reduce_near_piece(final, late)
            reduce_near(0)
            reduce_far(final - 1)
            reduce_far_piece(final, early)
        else:
            late = pieces - 1
            start_pass(final)
            end_pass(final)
            compute(final)
            reduce_near(final)
            reduce_near(0)
            reduce_far(final - 1)
            for p in range(pieces - 1):
                reduce_far_piece(final, p)
        first_contract = (((0,), (0,)), ((), ()))

        grad_blocks = full_width // grad_block
        middle = grad_blocks * 3 // 4
        for begin, end in ((0, middle), (middle, grad_blocks)):
            @pl.loop(begin, end)
            def _(b):
                cut = pl.ds(pl.multiple_of(b * grad_block, grad_block), grad_block)
                rows = full[:, 0, :, cut].reshape(total_rows, grad_block)
                gate_out[cut, :] = lax.dot_general(
                    rows, hid[0], first_contract, preferred_element_type=f32
                ).astype(bf16)
                up_out[cut, :] = lax.dot_general(
                    rows, hid[1], first_contract, preferred_element_type=f32
                ).astype(bf16)

            with jax.named_scope("S3"):
                if begin == 0:
                    reduce_far_piece(final, late)
                else:
                    reduce_far(0)
                    rets[me] = ret[me]

        @pl.loop(0, full_width // grad_block)
        def _(b):
            cut = pl.ds(pl.multiple_of(b * grad_block, grad_block), grad_block)
            grads = full[:, 1, :, cut].reshape(total_rows, grad_block)
            down_out[:, cut] = lax.dot_general(
                act[...], grads, first_contract, preferred_element_type=f32
            ).astype(bf16)

        @pl.loop(1, n)
        def _(k):
            j, i = k // span, k % span
            other = peer(j, i, 1)
            remote(ret.at[other], rets.at[other], bs.at[k], br.at[k], at(sp=other)).wait_recv()

        back = lax.dot_general(
            pick[...], rets[...].reshape(total_rows, width), first_contract,
            preferred_element_type=f32,
        )
        residual = (cot_ref[...].astype(f32) + back).astype(bf16)
        res_ref[...] = residual
        fullres_ref[:, mine] = residual

        def half_columns(member, h, q):
            start = member * width + h * half_width + q * quarter_width
            return pl.ds(pl.multiple_of(start, quarter_width), quarter_width)

        def half_of(h):
            return (1 - inner if h == 0 else inner) if halves == 2 else 0

        parts = [(h, q) for q in range(quarters) for h in range(halves)]

        def gather_copy(t, h, q):
            block = fullres_ref.at[:, half_columns(place, half_of(h), q)]
            to = partner if t == 0 else across(t, 1)
            return remote(block, block, gs.at[t, h, q], gr.at[t, h, q], at(tp=to))

        def gather_wait(t, h, q):
            origin = partner if t == 0 else across(t, -1)
            block = fullres_ref.at[:, half_columns(origin, half_of(h), q)]
            remote(block, block, gs.at[t, h, q], gr.at[t, h, q], at(tp=origin)).wait_recv()

        def gather_pass(t, h, q):
            block = fullres_ref.at[:, half_columns(across(t, -1), half_of(h), q)]
            return remote(block, block, hs.at[t, h, q], hr.at[t, h, q], at(tp=partner))

        def pass_wait(t, h, q):
            block = fullres_ref.at[
                :, half_columns(turned(t, -1) * 2 + (1 - core), half_of(h), q)
            ]
            remote(block, block, hs.at[t, h, q], hr.at[t, h, q], at(tp=partner)).wait_recv()

        for h, q in parts:
            for t in range(1, chips):
                gather_copy(t, h, q).start()
        for h, q in parts:
            gather_copy(0, h, q).start()

        def strip_at(other, q):
            start = pl.multiple_of(other * strip + q * slice_width, slice_width)
            if upright:
                return (slice(None), pl.ds(start, slice_width))
            return (pl.ds(start, slice_width), slice(None))

        def slice_at(q):
            cut = pl.ds(q * slice_width, slice_width)
            return (slice(None), cut) if upright else (cut, slice(None))

        def inner_peer(i, sign):
            return lax.rem(inner + sign * i + span, span)

        def outer_peer(g, sign):
            return lax.rem(group + sign * g + groups, groups)

        def inner_copy(g, i, q=0):
            other = outer_peer(g, 1) * span + inner_peer(i, 1)
            return remote(
                proj_part.at[strip_at(other, q)], proj_near.at[(g, i) + slice_at(q)],
                xs.at[g, i, q], xr.at[g, i, q], at(sp=group * span + inner_peer(i, 1)),
            )

        def outer_copy(g, q=0):
            return remote(
                proj_sum.at[(g,) + slice_at(q)], proj_far.at[(g,) + slice_at(q)],
                zs.at[g, q], zr.at[g, q], at(sp=outer_peer(g, 1) * span + inner),
            )

        turns = list(range(1, groups))
        turns = sorted(turns, key=lambda g: abs(g - groups // 2)) + [0]
        turn_width = span * strip

        def project(g):
            where = pl.ds(pl.multiple_of(outer_peer(g, 1) * turn_width, turn_width), turn_width)
            if upright:
                proj_part[:, where] = jnp.dot(
                    mix_ref[...], fullres_ref[:, where], preferred_element_type=f32
                ).astype(bf16)
            else:
                proj_part[where, :] = lax.dot_general(
                    fullres_ref[:, where], mix_ref[...], (((0,), (1,)), ((), ())),
                    preferred_element_type=f32,
                ).astype(bf16)
            for i in range(1, span):
                inner_copy(g, i).start()

        def turn_to(member):
            return lax.rem(member - group + groups, groups)

        def project_piece(member, h, q):
            where = half_columns(member, half_of(h), q)
            proj_part[:, where] = jnp.dot(
                mix_ref[...], fullres_ref[:, where], preferred_element_type=f32
            ).astype(bf16)
            if h == 0:
                inner_copy(turn_to(member), 1, q).start()

        def add_mix_grad(member, begin=False):
            where = columns(member)
            value = lax.dot_general(
                outp_ref[:, where], fullres_ref[:, where], (((1,), (1,)), ((), ())),
                preferred_element_type=f32,
            )
            mix_grad[...] = value if begin else mix_grad[...] + value

        def finish_inner(g, q=0):
            total_strip = proj_part[strip_at(outer_peer(g, 1) * span + inner, q)].astype(f32)
            for i in range(1, span):
                inner_copy(g, i, q).wait_recv()
                total_strip = total_strip + proj_near[(g, i) + slice_at(q)].astype(f32)
            proj_sum[(g,) + slice_at(q)] = total_strip.astype(bf16)

            @pl.when(g > 0)
            def _():
                outer_copy(g, q).start()

        far_side = turned(1, -1) * 2 + core
        far_pair = turned(1, -1) * 2 + (1 - core)
        if halves == 2:
            for q in range(quarters):
                for h in range(halves):
                    project_piece(place, h, q)
            add_mix_grad(place, True)
            for h, q in parts:
                gather_wait(0, h, q)
            for h in range(halves):
                project_piece(partner, h, 0)
            for q in range(quarters):
                for h in range(halves):
                    gather_wait(1, h, q)
                    gather_pass(1, h, q).start()
                    project_piece(far_side, h, q)
                    if q == 0 and h == 0:
                        add_mix_grad(partner)
                if q == 0:
                    for done in range(quarters):
                        finish_inner(turn_to(place), done)
                else:
                    finish_inner(turn_to(far_side), 0)
                    add_mix_grad(far_side)
                for h in range(halves):
                    pass_wait(1, h, q)
                    project_piece(far_pair, h, q)
                if q == 0:
                    for h in range(halves):
                        project_piece(partner, h, 1)
                    finish_inner(turn_to(partner), 0)
            add_mix_grad(far_pair)
        else:
            for t in range(1, chips):
                gather_wait(t, 0, 0)
                gather_pass(t, 0, 0).start()
            gather_wait(0, 0, 0)
            for t in range(1, chips):
                pass_wait(t, 0, 0)
            for g in turns[:2]:
                project(g)
        if halves == 1:
            mix_grad[...] = lax.dot_general(
                outp_ref[...], fullres_ref[...], (((1,), (1,)), ((), ())),
                preferred_element_type=f32,
            )
        lane = lax.broadcasted_iota(jnp.int32, (scan_rows, 128), 1)

        @pl.loop(0, channels // scan_rows)
        def _(b):
            rows = pl.ds(pl.multiple_of(b * scan_rows, scan_rows), scan_rows)
            upper = mix_grad[rows, :]
            branch_out[rows, :] = upper * gelu_slope[rows, :]
            grad = upper * gelu_val[rows, :]
            last = []
            for d in range(2):
                carried = decay[d, rows, :] * grad
                for level, by in enumerate(levels):
                    carried = carried + steps[d, level, rows, :] * shifted(carried, by, d)
                local[d, rows, :] = grad + jnp.where(inside(1, d, scan_rows), shifted(carried, 1, d), 0.0)
                last.append(carried[:, 0:1] if d == 0 else carried[:, length - 1 : length])
            packed_ends = jnp.where(lane == 0, last[0], jnp.where(lane == 1, last[1], 0.0))
            packed_ends = jnp.where(lane == 2, slopes[0, 3, rows, 0:128], packed_ends)
            ends[rows, :] = jnp.where(lane == 3, slopes[1, 3, rows, 0:128], packed_ends)

        if channels < channels_pad:
            ends[channels:, :] = jnp.zeros((channels_pad - channels, 128), f32)
        ends_row[...] = ends[...].T[0:8, :]

        def ends_copy(k):
            return remote(
                ends_row, ends_all.at[me], es.at[k], er.at[k], at(sp=lax.rem(me + k, n))
            )

        @pl.loop(1, n)
        def _(k):
            ends_copy(k).start()

        ends_all[me] = ends_row[...]

        if halves == 2:
            finish_inner(turn_to(far_pair), 0)
            finish_inner(turn_to(partner), 1)
            finish_inner(turn_to(far_side), 1)
            finish_inner(turn_to(far_pair), 1)
        else:
            for g in turns[2:]:
                project(g)
            for g in turns[:-2]:
                finish_inner(g)
        @pl.loop(1, n)
        def _(k):
            origin = lax.rem(me - k + n, n)
            remote(
                ends_row, ends_all.at[origin], es.at[k], er.at[k], at(sp=origin)
            ).wait_recv()

        incoming = [jnp.zeros((1, channels_pad), f32)] * 2
        for turn in range(n - 1):
            late = n - 1 - turn
            incoming[0] = jnp.where(
                late > me, ends_all[late, 2:3, :] * incoming[0] + ends_all[late, 0:1, :], incoming[0]
            )
            incoming[1] = jnp.where(
                turn < me, ends_all[turn, 3:4, :] * incoming[1] + ends_all[turn, 1:2, :], incoming[1]
            )
        line = lax.broadcasted_iota(jnp.int32, (128, channels_pad), 0)
        carry[...] = jnp.where(line == 0, incoming[0], jnp.where(line == 1, incoming[1], 0.0)).T

        @pl.loop(0, blocks)
        def _(b):
            rows = pl.ds(pl.multiple_of(b * block_width, block_width), block_width)
            value = jnp.zeros((block_width, length), f32)
            for d in range(2):
                delta = local[d, rows, :] + tails[d, rows, :] * carry[rows, d : d + 1]
                value = value + delta * slopes[d, 2, rows, :]
                value = value + jnp.dot(
                    wr_ref[d, b], (delta * slopes[d, 0, rows, :]).astype(bf16),
                    preferred_element_type=f32,
                )
                value = value + jnp.dot(
                    wi_ref[d, b], (delta * slopes[d, 1, rows, :]).astype(bf16),
                    preferred_element_type=f32,
                )
            conv_out[rows, :] = value

        if halves == 1:
            for g in turns[-2:]:
                finish_inner(g)
        summed = proj_sum[0].astype(f32)
        for g in turns[:-1]:
            for q in range(quarters):
                outer_copy(g, q).wait_recv()
            summed = summed + proj_far[g].astype(f32)
        proj_ref[...] = summed if upright else summed.T

        for g in turns:
            for q in range(quarters):
                for i in range(1, span):
                    inner_copy(g, i, q).wait_send()
                if g > 0:
                    outer_copy(g, q).wait_send()

        @pl.loop(1, n)
        def _(k):
            ends_copy(k).wait_send()

        @pl.loop(1, n)
        def _(k):
            j, i = k // span, k % span
            dispatch_copy(j, i, 1).wait_send()
            source = peer(j, i, -1)
            remote(ret.at[source], rets.at[me], bs.at[k], br.at[k], at(sp=source)).wait_send()

        @pl.loop(0, groups)
        def _(j):
            for i in range(fine):
                for copy in hand_over(j, i):
                    copy.wait_send()
                for t in range(1, chips):
                    pass_on(j, i, t).wait_send()
            for t in range(chips):
                if split_last:
                    for p in range(pieces):
                        @pl.when(j == groups - 1)
                        def _():
                            near_copy(j, t, p, 1).wait_send()

                    @pl.when(j < groups - 1)
                    def _():
                        near_copy(j, t).wait_send()
                else:
                    near_copy(j, t).wait_send()
            for t in range(1, chips):
                for p in range(pieces):
                    far_copy(j, t, p).wait_send()

        for h, q in parts:
            for t in range(chips):
                gather_copy(t, h, q).wait_send()
            for t in range(1, chips):
                gather_pass(t, h, q).wait_send()


    dma = pltpu.SemaphoreType.DMA
    wide = max(chips, 2)
    sem = lambda *shape: [dma(shape)] * 2
    any_spec = pl.BlockSpec(memory_space=pl.ANY)
    shape = jax.ShapeDtypeStruct
    strip_shape = (channels, strip) if upright else (strip, channels)
    part_shape = (channels, full_width) if upright else (full_width, channels)
    return pl.pallas_call(
        kernel, name="layer_backward",
        out_shape=(
            pltpu.VMEM((tokens, width), bf16), pltpu.VMEM((channels, strip), f32),
            pltpu.VMEM((channels, length), f32), pltpu.VMEM((channels, length), f32),
            pltpu.VMEM(w_gate.shape, bf16), pltpu.VMEM(w_up.shape, bf16), pltpu.VMEM(w_down.shape, bf16),
        ),
        in_specs=[VMEM_SPEC] * 13 + [any_spec] * 3,
        out_specs=(VMEM_SPEC,) * 7,
        scratch_shapes=[
            pltpu.VMEM(w_gate.shape, bf16), pltpu.VMEM(w_up.shape, bf16), pltpu.VMEM(w_down.shape, bf16),
            pltpu.VMEM((hidden, full_width), bf16), pltpu.VMEM((hidden, full_width), bf16),
            pltpu.VMEM((full_width, hidden), bf16),
            pltpu.VMEM((128, tokens), f32), pltpu.VMEM((128, tokens), f32),
            pltpu.VMEM((total_rows, tokens), bf16),
            pltpu.VMEM((n, 2, cap, width), bf16),
            pltpu.VMEM((n, 2, cap, full_width), bf16),
            pltpu.VMEM((2, total_rows, hidden), bf16),
            pltpu.VMEM((total_rows, hidden), bf16),
            pltpu.VMEM((total_rows, full_width), bf16),
            pltpu.VMEM((groups, chips, chunk, width), bf16),
            pltpu.VMEM((groups, chips, chunk, width), bf16),
            pltpu.VMEM((groups, chips, chunk, width), bf16),
            pltpu.VMEM((n, cap, width), bf16), pltpu.VMEM((n, cap, width), bf16),
            pltpu.VMEM((tokens, full_width), bf16),
            pltpu.VMEM((2, 4, channels, length), f32),
            pltpu.VMEM((2, len(levels), channels, length), f32),
            pltpu.VMEM((2, channels, length), f32), pltpu.VMEM((2, channels, length), f32),
            pltpu.VMEM((2, channels, 128), f32),
            pltpu.VMEM((channels, length), bf16),
            pltpu.VMEM((channels, length), f32), pltpu.VMEM((channels, length), f32),
            pltpu.VMEM((channels, length), f32), pltpu.VMEM((2, channels, length), f32),
            pltpu.VMEM((channels_pad, 128), f32), pltpu.VMEM((8, channels_pad), f32),
            pltpu.VMEM((n, 8, channels_pad), f32), pltpu.VMEM((channels_pad, 128), f32),
            pltpu.VMEM(part_shape, bf16),
            pltpu.VMEM((groups, span) + strip_shape, bf16),
            pltpu.VMEM((groups,) + strip_shape, bf16), pltpu.VMEM((groups,) + strip_shape, bf16),
        ]
        + sem(n) + sem(groups, span, quarters) + sem(groups, quarters)
        + [dma((3,))]
        + sem(n) + sem(units, wide) + sem(units) + sem(units, wide)
        + sem(groups, wide, pieces) + sem(groups, wide, pieces) + sem(n) + sem(wide, halves, quarters) + sem(wide, halves, quarters),
        compiler_params=pltpu.CompilerParams(
            collective_id=1, has_side_effects=True, vmem_limit_bytes=54 * 1024 * 1024
        ),
    )(
        cotangent, moe_input, routes.T, gates.T, conv_in, branch, state_before, state_after, jump,
        recur_weight, input_weight, lam, out_proj, w_gate, w_up, w_down,
    )


def write_out(values):
    count = len(values)

    def kernel(*refs):
        sems = refs[2 * count]
        copies = [
            pltpu.make_async_copy(refs[i], refs[count + i], sems.at[i]) for i in range(count)
        ]
        for copy in copies:
            copy.start()
        for copy in copies:
            copy.wait()

    return pl.pallas_call(
        kernel, name="write_out",
        out_shape=tuple(jax.ShapeDtypeStruct(v.shape, v.dtype) for v in values),
        in_specs=[pl.BlockSpec(memory_space=pl.ANY)] * count,
        out_specs=(pl.BlockSpec(memory_space=pl.ANY),) * count,
        scratch_shapes=[pltpu.SemaphoreType.DMA((count,))],
        compiler_params=pltpu.CompilerParams(vmem_limit_bytes=4 * 1024 * 1024),
    )(*values)


def on_device(
    cotangent, moe_input, routes, gates, w_gate, w_up, w_down, out_proj, conv_in, branch,
    state_before, state_after, jump, recur_weight, input_weight, lam,
):
    residual_grad, out_proj_grad, conv_grad, branch_grad, gate_grad, up_grad, down_grad = (
        write_out(layer_backward(
            cotangent, moe_input, routes, gates, w_gate[0], w_up[0], w_down[0], out_proj, conv_in,
            branch, state_before, state_after, jump, recur_weight, input_weight, lam,
        ))
    )
    return (
        gate_grad[None], up_grad[None], down_grad[None],
        residual_grad, out_proj_grad, conv_grad, branch_grad,
    )


def solution(mesh):
    placed = (
        P("sp", "tp"),
        P("sp", "tp"),
        P("sp", None),
        P("sp", None),
        P("sp", None, "tp"),
        P("sp", None, "tp"),
        P("sp", "tp", None),
        P("tp", None),
        P("tp", "sp"),
        P("tp", "sp"),
        P("tp", "sp"),
        P("tp", "sp"),
        P("tp", "sp"),
        P(None, "tp", None, None),
        P(None, "tp", None, None),
        P(None, "tp"),
    )
    return jax.shard_map(
        on_device,
        mesh=mesh,
        in_specs=placed,
        out_specs=(
            P("sp", None, "tp"),
            P("sp", None, "tp"),
            P("sp", "tp", None),
            P("sp", "tp"),
            P("tp", "sp"),
            P("tp", "sp"),
            P("tp", "sp"),
        ),
        check_vma=False,
    )
```

```python
import jax
import jax.numpy as jnp
from jax import lax
from jax.experimental import pallas as pl
from jax.experimental.pallas import tpu as pltpu
from jax.sharding import PartitionSpec as P

decay_scale = 8.0


MESH = pl.DeviceIdType.MESH
VMEM_SPEC = pl.BlockSpec(memory_space=pltpu.VMEM)


def at(sp=None, tp=None):
    sp = lax.axis_index("sp") if sp is None else sp
    tp = lax.axis_index("tp") if tp is None else tp
    return (sp, tp)


def greet(devices):
    barrier = pltpu.get_barrier_semaphore()
    for device in devices:
        pl.semaphore_signal(barrier, inc=1, device_id=device, device_id_type=MESH)


def await_greetings(count):
    pl.semaphore_wait(pltpu.get_barrier_semaphore(), count)


def remote(source, target, send, recv, device):
    return pltpu.make_async_remote_copy(
        src_ref=source, dst_ref=target, send_sem=send, recv_sem=recv,
        device_id=device, device_id_type=MESH,
    )


def softplus(value):
    small = jnp.exp(-jnp.abs(value))
    series = small * (1.0 - small * (0.5 - small * (1.0 / 3.0 - small * 0.25)))
    return jnp.maximum(value, 0.0) + jnp.where(small < 0.01, series, jnp.log(1.0 + small))


def one_minus_exp(value, exponential):
    series = -value * (
        1.0 + value * (0.5 + value * (1.0 / 6.0 + value * (1.0 / 24.0 + value * (
            1.0 / 120.0 + value * (1.0 / 720.0)
        ))))
    )
    return jnp.where(value > -0.25, series, 1.0 - exponential)


def layer_backward(
    cotangent, moe_input, routes, gates, w_gate, w_up, w_down, out_proj, conv_in, branch,
    state_before, state_after, jump, recur_weight, input_weight, lam,
):
    n, tp = lax.axis_size("sp"), lax.axis_size("tp")
    chips = tp // 2
    tokens, width = cotangent.shape
    full_width, hidden = w_gate.shape
    cap = -(-(3 * tokens // n) // 16) * 16
    span = min(n, 2 if n <= 8 else 4)
    groups = n // span
    fine = span if n <= 8 else 1
    per_unit = span // fine
    units = groups * fine
    chunk = span * cap
    total_rows = n * cap
    pieces = 2 if span % 2 == 0 else 1
    piece_rows, piece_sources = chunk // pieces, span // pieces
    split_last = fine == 2 and pieces == 2
    hidden_block = min(hidden, 256)
    column_block = min(full_width, 512)
    grad_block = min(full_width, 256)
    f32, bf16 = jnp.float32, jnp.bfloat16
    channels, length = conv_in.shape
    blocks, block_width = recur_weight.shape[1:3]
    channels_pad = max(channels, 128)
    strip = full_width // n
    upright = strip % 128 == 0
    halves = 2 if span == 2 and chips == 2 and groups == tp and upright else 1
    half_width = width // halves
    quarters = 2 if halves == 2 and strip % 256 == 0 else 1
    quarter_width, slice_width = half_width // quarters, strip // quarters
    scan_rows = min(channels, 128)
    levels = [1 << i for i in range((length - 1).bit_length())]

    def kernel(
        cot_ref, in_ref, routes_ref, gates_ref, conv_ref, branch_ref, before_ref, after_ref,
        jump_ref, wr_ref, wi_ref, lam_ref, outp_ref, wg_hbm, wu_hbm, wd_hbm,
        res_ref, proj_ref, conv_out, branch_out, gate_out, up_out, down_out,
        wg, wu, wd, wg_t, wu_t, wd_t, key_t, gate_t, pick, send, full, hid, act, part, near, total, far, ret, rets,
        fullres_ref,
        slopes, steps, decay, tails, speed, mix_ref, gelu_val, gelu_slope, mix_grad, local,
        ends, ends_row, ends_all, carry, proj_part, proj_near, proj_sum, proj_far,
        es, er, xs, xr, zs, zr,
        ws, ss, sr, ys, yr, ps, pr, fs, fr, ns, nr, ts, tr, bs, br, gs, gr, hs, hr,
    ):
        me, place = lax.axis_index("sp"), lax.axis_index("tp")
        chip, core = place // 2, place % 2
        partner = chip * 2 + (1 - core)
        group, inner = me // span, me % span

        def columns(member):
            return pl.ds(pl.multiple_of(member * width, width), width)

        mine = columns(place)

        def turned(t, sign):
            return lax.rem(chip + sign * t + chips, chips)

        def across(t, sign):
            return turned(t, sign) * 2 + core

        def order(j):
            return jnp.where(j < 2, j, groups + 1 - j)

        def group_of(j, sign):
            return lax.rem(group + sign * order(j) + groups, groups)

        def peer(j, i, sign):
            return group_of(j, sign) * span + lax.rem(inner + sign * i + span, span)

        weights = ((wg_hbm, wg), (wu_hbm, wu), (wd_hbm, wd))
        loads = [pltpu.make_async_copy(a, b, ws.at[i]) for i, (a, b) in enumerate(weights)]
        for load in loads:
            load.start()

        greet(
            [at(sp=lax.rem(me + k, n)) for k in range(1, n)]
            + [at(tp=partner)]
            + [at(tp=across(t, 1)) for t in range(1, chips)]
        )

        expert_id = lax.broadcasted_iota(jnp.int32, (128, tokens), 0)
        first = expert_id == routes_ref[0:1, :]
        second = expert_id == routes_ref[1:2, :]
        member = jnp.where(first | second, 1.0, 0.0).astype(f32)
        gate_t[...] = jnp.where(first, gates_ref[0:1, :], 0.0) + jnp.where(
            second, gates_ref[1:2, :], 0.0
        )
        earlier = lax.broadcasted_iota(jnp.int32, (tokens, tokens), 0) < lax.broadcasted_iota(
            jnp.int32, (tokens, tokens), 1
        )
        earlier = jnp.where(earlier, 1.0, 0.0).astype(bf16)
        position = jnp.dot(member.astype(bf16), earlier, preferred_element_type=f32)
        key_t[...] = jnp.where(member > 0.5, position, -1.0)
        row_id = lax.broadcasted_iota(jnp.int32, (cap, tokens), 0).astype(f32)

        def packed(to):
            chosen = row_id == key_t[pl.ds(to, 1), :]
            one_hot = jnp.where(chosen, 1.0, 0.0).astype(bf16)
            scale = jnp.sum(jnp.where(chosen, gate_t[pl.ds(to, 1), :], 0.0), axis=1, keepdims=True)
            pick[pl.ds(pl.multiple_of(to * cap, 16), cap), :] = one_hot
            rows = jnp.dot(one_hot, in_ref[...], preferred_element_type=f32).astype(bf16)
            grads = jnp.dot(one_hot, cot_ref[...], preferred_element_type=f32) * scale
            return rows, grads.astype(bf16)

        rows, grads = packed(me)
        full[me, 0, :, mine] = rows
        full[me, 1, :, mine] = grads

        def unit_slice(j, i):
            base = group_of(j, -1) * span
            if fine > 1:
                return pl.ds(base + lax.rem(inner - i + span, span), 1)
            return pl.ds(base, span)

        def dispatch_copy(j, i, sign):
            other = peer(j, i, sign)
            k = j * span + i
            return remote(
                send.at[other], full.at[me if sign > 0 else other, :, :, mine],
                ss.at[k], sr.at[k], at(sp=other),
            )

        def hand_over(j, i):
            block = full.at[unit_slice(j, i), :, :, mine]
            u = j * fine + i
            out = [
                remote(block, block, ys.at[u, t], yr.at[u, t], at(tp=across(t, 1)))
                for t in range(1, chips)
            ]
            out.append(remote(block, block, ps.at[u], pr.at[u], at(tp=partner)))
            return out

        def pass_on(j, i, t):
            block = full.at[unit_slice(j, i), :, :, columns(across(t, -1))]
            u = j * fine + i
            return remote(block, block, fs.at[u, t], fr.at[u, t], at(tp=partner))

        def start_forward(j, begin=0, end=fine):
            for i in range(begin, min(end, fine)):
                for s in range(per_unit):
                    number = i * per_unit + s

                    @pl.when(j * span + number > 0)
                    def _():
                        dispatch_copy(j, number, -1).wait_recv()

                for copy in hand_over(j, i):
                    copy.start()

        half = span // 2

        def release(j, begin, end):
            @pl.when(j < groups)
            def _():
                for i in range(begin, end):
                    dispatch_copy(j, i, 1).start()

        def start_pass(j, begin=0, end=fine):
            for i in range(begin, end):
                u = j * fine + i
                for t in range(1, chips):
                    block = full.at[unit_slice(j, i), :, :, columns(across(t, -1))]
                    remote(
                        block, block, ys.at[u, t], yr.at[u, t], at(tp=across(t, -1))
                    ).wait_recv()
                    pass_on(j, i, t).start()

        def end_pass(j, begin=0, end=fine):
            for i in range(begin, end):
                u = j * fine + i
                block = full.at[unit_slice(j, i), :, :, columns(partner)]
                remote(block, block, ps.at[u], pr.at[u], at(tp=partner)).wait_recv()
                for t in range(1, chips):
                    block = full.at[
                        unit_slice(j, i), :, :, columns(turned(t, -1) * 2 + (1 - core))
                    ]
                    remote(block, block, fs.at[u, t], fr.at[u, t], at(tp=partner)).wait_recv()

        def chunk_rows(j):
            return pl.ds(pl.multiple_of(group_of(j, -1) * chunk, 16), chunk)

        def near_copy(j, t, p=0, count=pieces):
            base = group_of(j, -1) * chunk
            rows = pl.ds(pl.multiple_of(base + p * piece_rows, 16), count * piece_rows)
            return remote(
                part.at[rows, columns(turned(t, 1) * 2 + (1 - core))],
                near.at[j, t, piece(p, count)], ns.at[j, t, p], nr.at[j, t, p], at(tp=partner),
            )

        def piece(p, count=1):
            return pl.ds(pl.multiple_of(p * piece_rows, 16), count * piece_rows)

        def far_copy(j, t, i):
            return remote(
                total.at[j, t, piece(i)], far.at[j, t, piece(i)],
                ts.at[j, t, i], tr.at[j, t, i], at(tp=across(t, 1)),
            )

        def compute(j, p=0, count=pieces):
            base = group_of(j, -1)
            size = count * piece_rows
            where = pl.ds(pl.multiple_of(base * chunk + p * piece_rows, 16), size)
            sources = pl.ds(base * span + p * piece_sources, count * piece_sources)

            @pl.loop(0, hidden // hidden_block)
            def _(b):
                cut = pl.ds(pl.multiple_of(b * hidden_block, hidden_block), hidden_block)
                rows = full[sources, 0].reshape(size, full_width)
                pre_gate = jnp.dot(rows, wg[:, cut], preferred_element_type=f32)
                pre_up = jnp.dot(rows, wu[:, cut], preferred_element_type=f32)
                grads = full[sources, 1].reshape(size, full_width)
                act_grad = jnp.dot(grads, wd_t[:, cut], preferred_element_type=f32)
                sigmoid = jax.nn.sigmoid(pre_gate)
                silu = pre_gate * sigmoid
                slope = sigmoid * (1.0 + pre_gate * (1.0 - sigmoid))
                act[where, cut] = (silu * pre_up).astype(bf16)
                hid[0, where, cut] = (act_grad * pre_up * slope).astype(bf16)
                hid[1, where, cut] = (act_grad * silu).astype(bf16)

            @pl.loop(0, chips)
            def _(turn):
                t = lax.rem(turn + 1, chips)
                for side in ((1 - core), core):
                    cut = columns(turned(t, 1) * 2 + side)
                    value = jnp.dot(
                        hid[0, where, :], wg_t[:, cut], preferred_element_type=f32
                    ) + jnp.dot(hid[1, where, :], wu_t[:, cut], preferred_element_type=f32)
                    part[where, cut] = value.astype(bf16)
                    if side is not core:
                        near_copy(j, t, p, count).start()

        def add_near(j, t, p):
            where = pl.ds(pl.multiple_of(group_of(j, -1) * chunk + p * piece_rows, 16), piece_rows)
            value = part[where, columns(turned(t, 1) * 2 + core)].astype(f32) + near[
                j, t, piece(p)
            ].astype(f32)
            total[j, t, piece(p)] = value.astype(bf16)
            far_copy(j, t, p).start()

        def reduce_near(j):
            for t in list(range(1, chips)) + [0]:
                near_copy(j, t).wait_recv()
                if t > 0:
                    for p in range(pieces):
                        add_near(j, t, p)

        def reduce_near_piece(j, p):
            for t in list(range(1, chips)) + [0]:
                near_copy(j, t, p, 1).wait_recv()
                if t > 0:
                    add_near(j, t, p)

        def return_copy(j, source):
            turn = lax.rem(inner - source + span, span)
            k = j * span + turn
            other = group_of(j, -1) * span + source
            return k, remote(ret.at[other], rets.at[me], bs.at[k], br.at[k], at(sp=other))

        def reduce_far_piece(j, p):
            base = group_of(j, -1)
            where = pl.ds(pl.multiple_of(base * chunk + p * piece_rows, 16), piece_rows)
            value = part[where, mine].astype(f32) + near[j, 0, piece(p)].astype(f32)
            for t in range(1, chips):
                far_copy(j, t, p).wait_recv()
                value = value + far[j, t, piece(p)].astype(f32)
            ret[pl.ds(base * span + p * piece_sources, piece_sources)] = value.astype(
                bf16
            ).reshape(piece_sources, cap, width)
            for s in range(piece_sources):
                k, copy = return_copy(j, p * piece_sources + s)

                @pl.when(k > 0)
                def _():
                    copy.start()

        def reduce_far(j):
            for p in range(pieces):
                reduce_far_piece(j, p)

        @pl.loop(1, n)
        def _(k):
            to = peer(k // span, k % span, 1)
            rows, grads = packed(to)
            send[to, 0] = rows
            send[to, 1] = grads

        await_greetings(n + chips - 1)
        if fine > 1:
            for copy in hand_over(0, 0):
                copy.start()

        @pl.loop(1, span + half)
        def _(k):
            dispatch_copy(k // span, k % span, 1).start()

        for load in loads:
            load.wait()

        @pl.loop(0, full_width // grad_block)
        def _(b):
            cut = pl.ds(pl.multiple_of(b * grad_block, grad_block), grad_block)
            wd_t[cut, :] = wd[:, cut].T
            wg_t[:, cut] = wg[cut, :].T
            wu_t[:, cut] = wu[cut, :].T

        release(1, half, span)
        start_forward(0, 1 if fine > 1 else 0)
        release(2, 0, span)

        diagonal = lax.broadcasted_iota(jnp.int32, (channels, channels), 0) == (
            lax.broadcasted_iota(jnp.int32, (channels, channels), 1)
        )
        for d in range(2):
            column = jnp.sum(
                jnp.where(diagonal, lam_ref[d : d + 1, :], 0.0), axis=1, keepdims=True
            )
            speed[d] = decay_scale * softplus(-jnp.broadcast_to(column, (channels, 128)))

        def shifted(value, by, d):
            return pltpu.roll(value, length - by if d == 0 else by, 1)

        def inside(by, d, rows=block_width):
            token = lax.broadcasted_iota(jnp.int32, (rows, length), 1)
            return token < length - by if d == 0 else token >= by

        @pl.loop(0, blocks)
        def _(b):
            rows = pl.ds(pl.multiple_of(b * block_width, block_width), block_width)
            conv = conv_ref[rows, :]
            wide = conv.astype(f32)
            lru_out = jnp.zeros((block_width, length), f32)
            for d, state_ref in enumerate((before_ref, after_ref)):
                recur = jax.nn.sigmoid(
                    lax.dot_general(
                        wr_ref[d, b], conv, (((0,), (0,)), ((), ())), preferred_element_type=f32
                    )
                )
                inward = jax.nn.sigmoid(
                    lax.dot_general(
                        wi_ref[d, b], conv, (((0,), (0,)), ((), ())), preferred_element_type=f32
                    )
                )
                rate = speed[d, rows, 0:1]
                log_decay = jump_ref[rows, :] - rate * recur
                retain = jnp.exp(log_decay)
                root = jnp.sqrt(one_minus_exp(2.0 * log_decay, retain * retain))
                state = state_ref[rows, :]
                lru_out = lru_out + retain * state + root * inward * wide
                log_slope = state * retain - inward * wide * retain * retain / root
                slopes[d, 0, rows, :] = -rate * log_slope * recur * (1.0 - recur)
                slopes[d, 1, rows, :] = root * wide * inward * (1.0 - inward)
                slopes[d, 2, rows, :] = root * inward
                decay[d, rows, :] = retain
                product = retain
                for level, by in enumerate(levels):
                    keep = inside(by, d)
                    steps[d, level, rows, :] = jnp.where(keep, product, 0.0)
                    product = product * jnp.where(keep, shifted(product, by, d), 1.0)
                tails[d, rows, :] = jnp.where(inside(1, d), shifted(product, 1, d), 1.0)
                slopes[d, 3, rows, 0:128] = jnp.broadcast_to(
                    product[:, 0:1] if d == 0 else product[:, length - 1 : length],
                    (block_width, 128),
                )
            value = branch_ref[rows, :].astype(f32)
            scale = 0.7978845608028654
            tanh = jnp.tanh(scale * (value + 0.044715 * value * value * value))
            half = 0.5 * (1.0 + tanh)
            gelu = value * half
            slope = half + 0.5 * value * (1.0 - tanh * tanh) * scale * (
                1.0 + 3.0 * 0.044715 * value * value
            )
            mix_ref[rows, :] = (lru_out * gelu).astype(bf16)
            gelu_val[rows, :] = gelu
            gelu_slope[rows, :] = lru_out * slope


        @pl.loop(0, groups - 1)
        def _(j):
            @pl.when(j < groups - 2)
            def _():
                start_forward(j + 1)
                release(j + 3, 0, half)

            @pl.when((j > 0) & (j < groups - 2))
            def _():
                release(j + 2, half, span)

            start_pass(j)
            end_pass(j)
            compute(j)

            @pl.when(j == groups - 2)
            def _():
                start_forward(groups - 1, 1)

            @pl.when(j > 0)
            def _():
                reduce_near(j)

            @pl.when(j == groups - 3)
            def _():
                start_forward(groups - 1, 0, 1)

            @pl.when(j > 1)
            def _():
                reduce_far(j - 1)

        final = groups - 1
        if split_last:
            early, late = lax.rem(inner + span, span), lax.rem(inner + span - 1, span)
            start_pass(final, 0, 1)
            end_pass(final, 0, 1)
            compute(final, early, 1)
            start_pass(final, 1)
            reduce_near_piece(final, early)
            end_pass(final, 1)
            compute(final, late, 1)
            reduce_near_piece(final, late)
            reduce_near(0)
            reduce_far(final - 1)
            reduce_far_piece(final, early)
        else:
            late = pieces - 1
            start_pass(final)
            end_pass(final)
            compute(final)
            reduce_near(final)
            reduce_near(0)
            reduce_far(final - 1)
            for p in range(pieces - 1):
                reduce_far_piece(final, p)
        first_contract = (((0,), (0,)), ((), ()))

        grad_blocks = full_width // grad_block
        middle = grad_blocks * 3 // 4
        for begin, end in ((0, middle), (middle, grad_blocks)):
            @pl.loop(begin, end)
            def _(b):
                cut = pl.ds(pl.multiple_of(b * grad_block, grad_block), grad_block)
                rows = full[:, 0, :, cut].reshape(total_rows, grad_block)
                gate_out[cut, :] = lax.dot_general(
                    rows, hid[0], first_contract, preferred_element_type=f32
                ).astype(bf16)
                up_out[cut, :] = lax.dot_general(
                    rows, hid[1], first_contract, preferred_element_type=f32
                ).astype(bf16)

            with jax.named_scope("S3"):
                if begin == 0:
                    reduce_far_piece(final, late)
                else:
                    reduce_far(0)
                    rets[me] = ret[me]

        @pl.loop(0, full_width // grad_block)
        def _(b):
            cut = pl.ds(pl.multiple_of(b * grad_block, grad_block), grad_block)
            grads = full[:, 1, :, cut].reshape(total_rows, grad_block)
            down_out[:, cut] = lax.dot_general(
                act[...], grads, first_contract, preferred_element_type=f32
            ).astype(bf16)

        @pl.loop(1, n)
        def _(k):
            j, i = k // span, k % span
            other = peer(j, i, 1)
            remote(ret.at[other], rets.at[other], bs.at[k], br.at[k], at(sp=other)).wait_recv()

        back = lax.dot_general(
            pick[...], rets[...].reshape(total_rows, width), first_contract,
            preferred_element_type=f32,
        )
        residual = (cot_ref[...].astype(f32) + back).astype(bf16)
        res_ref[...] = residual
        fullres_ref[:, mine] = residual

        def half_columns(member, h, q):
            start = member * width + h * half_width + q * quarter_width
            return pl.ds(pl.multiple_of(start, quarter_width), quarter_width)

        def half_of(h):
            return (1 - inner if h == 0 else inner) if halves == 2 else 0

        parts = [(h, q) for q in range(quarters) for h in range(halves)]

        def gather_copy(t, h, q):
            block = fullres_ref.at[:, half_columns(place, half_of(h), q)]
            to = partner if t == 0 else across(t, 1)
            return remote(block, block, gs.at[t, h, q], gr.at[t, h, q], at(tp=to))

        def gather_wait(t, h, q):
            origin = partner if t == 0 else across(t, -1)
            block = fullres_ref.at[:, half_columns(origin, half_of(h), q)]
            remote(block, block, gs.at[t, h, q], gr.at[t, h, q], at(tp=origin)).wait_recv()

        def gather_pass(t, h, q):
            block = fullres_ref.at[:, half_columns(across(t, -1), half_of(h), q)]
            return remote(block, block, hs.at[t, h, q], hr.at[t, h, q], at(tp=partner))

        def pass_wait(t, h, q):
            block = fullres_ref.at[
                :, half_columns(turned(t, -1) * 2 + (1 - core), half_of(h), q)
            ]
            remote(block, block, hs.at[t, h, q], hr.at[t, h, q], at(tp=partner)).wait_recv()

        for h, q in parts:
            for t in range(1, chips):
                gather_copy(t, h, q).start()
        for h, q in parts:
            gather_copy(0, h, q).start()

        def strip_at(other, q):
            start = pl.multiple_of(other * strip + q * slice_width, slice_width)
            if upright:
                return (slice(None), pl.ds(start, slice_width))
            return (pl.ds(start, slice_width), slice(None))

        def slice_at(q):
            cut = pl.ds(q * slice_width, slice_width)
            return (slice(None), cut) if upright else (cut, slice(None))

        def inner_peer(i, sign):
            return lax.rem(inner + sign * i + span, span)

        def outer_peer(g, sign):
            return lax.rem(group + sign * g + groups, groups)

        def inner_copy(g, i, q=0):
            other = outer_peer(g, 1) * span + inner_peer(i, 1)
            return remote(
                proj_part.at[strip_at(other, q)], proj_near.at[(g, i) + slice_at(q)],
                xs.at[g, i, q], xr.at[g, i, q], at(sp=group * span + inner_peer(i, 1)),
            )

        def outer_copy(g, q=0):
            return remote(
                proj_sum.at[(g,) + slice_at(q)], proj_far.at[(g,) + slice_at(q)],
                zs.at[g, q], zr.at[g, q], at(sp=outer_peer(g, 1) * span + inner),
            )

        turns = list(range(1, groups))
        turns = sorted(turns, key=lambda g: abs(g - groups // 2)) + [0]
        turn_width = span * strip

        def project(g):
            where = pl.ds(pl.multiple_of(outer_peer(g, 1) * turn_width, turn_width), turn_width)
            if upright:
                proj_part[:, where] = jnp.dot(
                    mix_ref[...], fullres_ref[:, where], preferred_element_type=f32
                ).astype(bf16)
            else:
                proj_part[where, :] = lax.dot_general(
                    fullres_ref[:, where], mix_ref[...], (((0,), (1,)), ((), ())),
                    preferred_element_type=f32,
                ).astype(bf16)
            for i in range(1, span):
                inner_copy(g, i).start()

        def turn_to(member):
            return lax.rem(member - group + groups, groups)

        def project_piece(member, h, q):
            where = half_columns(member, half_of(h), q)
            proj_part[:, where] = jnp.dot(
                mix_ref[...], fullres_ref[:, where], preferred_element_type=f32
            ).astype(bf16)
            if h == 0:
                inner_copy(turn_to(member), 1, q).start()

        def add_mix_grad(member, begin=False):
            where = columns(member)
            value = lax.dot_general(
                outp_ref[:, where], fullres_ref[:, where], (((1,), (1,)), ((), ())),
                preferred_element_type=f32,
            )
            mix_grad[...] = value if begin else mix_grad[...] + value

        def finish_inner(g, q=0):
            total_strip = proj_part[strip_at(outer_peer(g, 1) * span + inner, q)].astype(f32)
            for i in range(1, span):
                inner_copy(g, i, q).wait_recv()
                total_strip = total_strip + proj_near[(g, i) + slice_at(q)].astype(f32)
            proj_sum[(g,) + slice_at(q)] = total_strip.astype(bf16)

            @pl.when(g > 0)
            def _():
                outer_copy(g, q).start()

        far_side = turned(1, -1) * 2 + core
        far_pair = turned(1, -1) * 2 + (1 - core)
        if halves == 2:
            for q in range(quarters):
                for h in range(halves):
                    project_piece(place, h, q)
            add_mix_grad(place, True)
            for h, q in parts:
                gather_wait(0, h, q)
            for q in range(quarters):
                for h in range(halves):
                    gather_wait(1, h, q)
                    gather_pass(1, h, q).start()
                    project_piece(far_side, h, q)
                    if q == 0 and h == 0:
                        add_mix_grad(partner)
                if q == 0:
                    for done in range(quarters):
                        finish_inner(turn_to(place), done)
                else:
                    finish_inner(turn_to(far_side), 0)
                    add_mix_grad(far_side)
                for h in range(halves):
                    pass_wait(1, h, q)
                    project_piece(far_pair, h, q)
                if q == 0:
                    for r in range(quarters):
                        for h in range(halves):
                            project_piece(partner, h, r)
            add_mix_grad(far_pair)
        else:
            for t in range(1, chips):
                gather_wait(t, 0, 0)
                gather_pass(t, 0, 0).start()
            gather_wait(0, 0, 0)
            for t in range(1, chips):
                pass_wait(t, 0, 0)
            for g in turns[:2]:
                project(g)
        if halves == 1:
            mix_grad[...] = lax.dot_general(
                outp_ref[...], fullres_ref[...], (((1,), (1,)), ((), ())),
                preferred_element_type=f32,
            )
        lane = lax.broadcasted_iota(jnp.int32, (scan_rows, 128), 1)

        @pl.loop(0, channels // scan_rows)
        def _(b):
            rows = pl.ds(pl.multiple_of(b * scan_rows, scan_rows), scan_rows)
            upper = mix_grad[rows, :]
            branch_out[rows, :] = upper * gelu_slope[rows, :]
            grad = upper * gelu_val[rows, :]
            last = []
            for d in range(2):
                carried = decay[d, rows, :] * grad
                for level, by in enumerate(levels):
                    carried = carried + steps[d, level, rows, :] * shifted(carried, by, d)
                local[d, rows, :] = grad + jnp.where(inside(1, d, scan_rows), shifted(carried, 1, d), 0.0)
                last.append(carried[:, 0:1] if d == 0 else carried[:, length - 1 : length])
            packed_ends = jnp.where(lane == 0, last[0], jnp.where(lane == 1, last[1], 0.0))
            packed_ends = jnp.where(lane == 2, slopes[0, 3, rows, 0:128], packed_ends)
            ends[rows, :] = jnp.where(lane == 3, slopes[1, 3, rows, 0:128], packed_ends)

        if channels < channels_pad:
            ends[channels:, :] = jnp.zeros((channels_pad - channels, 128), f32)
        ends_row[...] = ends[...].T[0:8, :]

        def ends_copy(k):
            return remote(
                ends_row, ends_all.at[me], es.at[k], er.at[k], at(sp=lax.rem(me + k, n))
            )

        @pl.loop(1, n)
        def _(k):
            ends_copy(k).start()

        ends_all[me] = ends_row[...]

        if halves == 2:
            finish_inner(turn_to(far_pair), 0)
            finish_inner(turn_to(partner), 0)
            finish_inner(turn_to(partner), 1)
            finish_inner(turn_to(far_side), 1)
            finish_inner(turn_to(far_pair), 1)
        else:
            for g in turns[2:]:
                project(g)
            for g in turns[:-2]:
                finish_inner(g)
        @pl.loop(1, n)
        def _(k):
            origin = lax.rem(me - k + n, n)
            remote(
                ends_row, ends_all.at[origin], es.at[k], er.at[k], at(sp=origin)
            ).wait_recv()

        incoming = [jnp.zeros((1, channels_pad), f32)] * 2
        for turn in range(n - 1):
            late = n - 1 - turn
            incoming[0] = jnp.where(
                late > me, ends_all[late, 2:3, :] * incoming[0] + ends_all[late, 0:1, :], incoming[0]
            )
            incoming[1] = jnp.where(
                turn < me, ends_all[turn, 3:4, :] * incoming[1] + ends_all[turn, 1:2, :], incoming[1]
            )
        line = lax.broadcasted_iota(jnp.int32, (128, channels_pad), 0)
        carry[...] = jnp.where(line == 0, incoming[0], jnp.where(line == 1, incoming[1], 0.0)).T

        @pl.loop(0, blocks)
        def _(b):
            rows = pl.ds(pl.multiple_of(b * block_width, block_width), block_width)
            value = jnp.zeros((block_width, length), f32)
            for d in range(2):
                delta = local[d, rows, :] + tails[d, rows, :] * carry[rows, d : d + 1]
                value = value + delta * slopes[d, 2, rows, :]
                value = value + jnp.dot(
                    wr_ref[d, b], (delta * slopes[d, 0, rows, :]).astype(bf16),
                    preferred_element_type=f32,
                )
                value = value + jnp.dot(
                    wi_ref[d, b], (delta * slopes[d, 1, rows, :]).astype(bf16),
                    preferred_element_type=f32,
                )
            conv_out[rows, :] = value

        if halves == 1:
            for g in turns[-2:]:
                finish_inner(g)
        summed = proj_sum[0].astype(f32)
        for g in turns[:-1]:
            for q in range(quarters):
                outer_copy(g, q).wait_recv()
            summed = summed + proj_far[g].astype(f32)
        proj_ref[...] = summed if upright else summed.T

        for g in turns:
            for q in range(quarters):
                for i in range(1, span):
                    inner_copy(g, i, q).wait_send()
                if g > 0:
                    outer_copy(g, q).wait_send()

        @pl.loop(1, n)
        def _(k):
            ends_copy(k).wait_send()

        @pl.loop(1, n)
        def _(k):
            j, i = k // span, k % span
            dispatch_copy(j, i, 1).wait_send()
            source = peer(j, i, -1)
            remote(ret.at[source], rets.at[me], bs.at[k], br.at[k], at(sp=source)).wait_send()

        @pl.loop(0, groups)
        def _(j):
            for i in range(fine):
                for copy in hand_over(j, i):
                    copy.wait_send()
                for t in range(1, chips):
                    pass_on(j, i, t).wait_send()
            for t in range(chips):
                if split_last:
                    for p in range(pieces):
                        @pl.when(j == groups - 1)
                        def _():
                            near_copy(j, t, p, 1).wait_send()

                    @pl.when(j < groups - 1)
                    def _():
                        near_copy(j, t).wait_send()
                else:
                    near_copy(j, t).wait_send()
            for t in range(1, chips):
                for p in range(pieces):
                    far_copy(j, t, p).wait_send()

        for h, q in parts:
            for t in range(chips):
                gather_copy(t, h, q).wait_send()
            for t in range(1, chips):
                gather_pass(t, h, q).wait_send()


    dma = pltpu.SemaphoreType.DMA
    wide = max(chips, 2)
    sem = lambda *shape: [dma(shape)] * 2
    any_spec = pl.BlockSpec(memory_space=pl.ANY)
    shape = jax.ShapeDtypeStruct
    strip_shape = (channels, strip) if upright else (strip, channels)
    part_shape = (channels, full_width) if upright else (full_width, channels)
    return pl.pallas_call(
        kernel, name="layer_backward",
        out_shape=(
            pltpu.VMEM((tokens, width), bf16), pltpu.VMEM((channels, strip), f32),
            pltpu.VMEM((channels, length), f32), pltpu.VMEM((channels, length), f32),
            pltpu.VMEM(w_gate.shape, bf16), pltpu.VMEM(w_up.shape, bf16), pltpu.VMEM(w_down.shape, bf16),
        ),
        in_specs=[VMEM_SPEC] * 13 + [any_spec] * 3,
        out_specs=(VMEM_SPEC,) * 7,
        scratch_shapes=[
            pltpu.VMEM(w_gate.shape, bf16), pltpu.VMEM(w_up.shape, bf16), pltpu.VMEM(w_down.shape, bf16),
            pltpu.VMEM((hidden, full_width), bf16), pltpu.VMEM((hidden, full_width), bf16),
            pltpu.VMEM((full_width, hidden), bf16),
            pltpu.VMEM((128, tokens), f32), pltpu.VMEM((128, tokens), f32),
            pltpu.VMEM((total_rows, tokens), bf16),
            pltpu.VMEM((n, 2, cap, width), bf16),
            pltpu.VMEM((n, 2, cap, full_width), bf16),
            pltpu.VMEM((2, total_rows, hidden), bf16),
            pltpu.VMEM((total_rows, hidden), bf16),
            pltpu.VMEM((total_rows, full_width), bf16),
            pltpu.VMEM((groups, chips, chunk, width), bf16),
            pltpu.VMEM((groups, chips, chunk, width), bf16),
            pltpu.VMEM((groups, chips, chunk, width), bf16),
            pltpu.VMEM((n, cap, width), bf16), pltpu.VMEM((n, cap, width), bf16),
            pltpu.VMEM((tokens, full_width), bf16),
            pltpu.VMEM((2, 4, channels, length), f32),
            pltpu.VMEM((2, len(levels), channels, length), f32),
            pltpu.VMEM((2, channels, length), f32), pltpu.VMEM((2, channels, length), f32),
            pltpu.VMEM((2, channels, 128), f32),
            pltpu.VMEM((channels, length), bf16),
            pltpu.VMEM((channels, length), f32), pltpu.VMEM((channels, length), f32),
            pltpu.VMEM((channels, length), f32), pltpu.VMEM((2, channels, length), f32),
            pltpu.VMEM((channels_pad, 128), f32), pltpu.VMEM((8, channels_pad), f32),
            pltpu.VMEM((n, 8, channels_pad), f32), pltpu.VMEM((channels_pad, 128), f32),
            pltpu.VMEM(part_shape, bf16),
            pltpu.VMEM((groups, span) + strip_shape, bf16),
            pltpu.VMEM((groups,) + strip_shape, bf16), pltpu.VMEM((groups,) + strip_shape, bf16),
        ]
        + sem(n) + sem(groups, span, quarters) + sem(groups, quarters)
        + [dma((3,))]
        + sem(n) + sem(units, wide) + sem(units) + sem(units, wide)
        + sem(groups, wide, pieces) + sem(groups, wide, pieces) + sem(n) + sem(wide, halves, quarters) + sem(wide, halves, quarters),
        compiler_params=pltpu.CompilerParams(
            collective_id=1, has_side_effects=True, vmem_limit_bytes=54 * 1024 * 1024
        ),
    )(
        cotangent, moe_input, routes.T, gates.T, conv_in, branch, state_before, state_after, jump,
        recur_weight, input_weight, lam, out_proj, w_gate, w_up, w_down,
    )


def write_out(values):
    count = len(values)

    def kernel(*refs):
        sems = refs[2 * count]
        copies = [
            pltpu.make_async_copy(refs[i], refs[count + i], sems.at[i]) for i in range(count)
        ]
        for copy in copies:
            copy.start()
        for copy in copies:
            copy.wait()

    return pl.pallas_call(
        kernel, name="write_out",
        out_shape=tuple(jax.ShapeDtypeStruct(v.shape, v.dtype) for v in values),
        in_specs=[pl.BlockSpec(memory_space=pl.ANY)] * count,
        out_specs=(pl.BlockSpec(memory_space=pl.ANY),) * count,
        scratch_shapes=[pltpu.SemaphoreType.DMA((count,))],
        compiler_params=pltpu.CompilerParams(vmem_limit_bytes=4 * 1024 * 1024),
    )(*values)


def on_device(
    cotangent, moe_input, routes, gates, w_gate, w_up, w_down, out_proj, conv_in, branch,
    state_before, state_after, jump, recur_weight, input_weight, lam,
):
    residual_grad, out_proj_grad, conv_grad, branch_grad, gate_grad, up_grad, down_grad = (
        write_out(layer_backward(
            cotangent, moe_input, routes, gates, w_gate[0], w_up[0], w_down[0], out_proj, conv_in,
            branch, state_before, state_after, jump, recur_weight, input_weight, lam,
        ))
    )
    return (
        gate_grad[None], up_grad[None], down_grad[None],
        residual_grad, out_proj_grad, conv_grad, branch_grad,
    )


def solution(mesh):
    placed = (
        P("sp", "tp"),
        P("sp", "tp"),
        P("sp", None),
        P("sp", None),
        P("sp", None, "tp"),
        P("sp", None, "tp"),
        P("sp", "tp", None),
        P("tp", None),
        P("tp", "sp"),
        P("tp", "sp"),
        P("tp", "sp"),
        P("tp", "sp"),
        P("tp", "sp"),
        P(None, "tp", None, None),
        P(None, "tp", None, None),
        P(None, "tp"),
    )
    return jax.shard_map(
        on_device,
        mesh=mesh,
        in_specs=placed,
        out_specs=(
            P("sp", None, "tp"),
            P("sp", None, "tp"),
            P("sp", "tp", None),
            P("sp", "tp"),
            P("tp", "sp"),
            P("tp", "sp"),
            P("tp", "sp"),
        ),
        check_vma=False,
    )
```
